32 devices in a mesh: rep: 2 (over x), fs: 8 (over z, y), tp: 2 (over core).
Axes of the slice: x: 2, y: 2, z: 4, core: 2. Of those that a mesh axis runs over, the one named last changes fastest.
Arguments:
- late_rows: bfloat16 [4096, 2048], P(('rep', 'fs')), parts along dimension 0, may hold values from -6 to 6
- early_rows: bfloat16 [4096, 2048], P(('rep', 'fs')), parts along dimension 0, may hold values from -6 to 6
- hidden_cot: bfloat16 [4096, 5632], P(('rep', 'fs'), 'tp'), parts along dimension 0, may hold values from -6 to 6
- gate_weight: bfloat16 [2048, 5632], P('fs', 'tp'), may hold values from -0.125 to 0.125
- up_weight: bfloat16 [2048, 5632], P('fs', 'tp'), may hold values from -0.125 to 0.125
- gate_taps: bfloat16 [3, 5632], P(None, 'tp'), may hold values from -3.5 to 3.5
- up_taps: bfloat16 [3, 5632], P(None, 'tp'), may hold values from -3.5 to 3.5
- gate_grad_sum: float32 [4096, 5632], P(('rep', 'fs'), 'tp'), parts along dimension 0, may hold values from -6 to 6
- up_grad_sum: float32 [4096, 5632], P(('rep', 'fs'), 'tp'), parts along dimension 0, may hold values from -6 to 6
- gate_taps_sum: float32 [6, 5632], P('rep', 'tp'), parts along dimension 0, may hold values from -6 to 6
- up_taps_sum: float32 [6, 5632], P('rep', 'tp'), parts along dimension 0, may hold values from -6 to 6
Outputs:
- late_hidden: bfloat16 [4096, 5632], P(('rep', 'fs'), 'tp'), parts along dimension 0
- early_grad: bfloat16 [4096, 2048], P(('rep', 'fs')), parts along dimension 0
- gate_grad_next: float32 [4096, 5632], P(('rep', 'fs'), 'tp'), parts along dimension 0
- up_grad_next: float32 [4096, 5632], P(('rep', 'fs'), 'tp'), parts along dimension 0
- gate_taps_next: float32 [6, 5632], P('rep', 'tp'), parts along dimension 0
- up_taps_next: float32 [6, 5632], P('rep', 'tp'), parts along dimension 0
The draws below stay inside these ranges and needn't reach their ends.
There are 2 independent parts, one for each index of `rep`. The reference program is written for one: setup_inputs(seed, part) draws one part's arguments, and reference() takes and returns one part's arrays. A program takes and returns all parts, laid end to end along the dimension named above; an argument that names none is the same for every part. Nothing has to cross between parts.
All inputs are finite; a program needn't handle non-finite values.
Results may differ from the reference program's by a relative error of at most 0.02.
Values may be sent and summed in bfloat16 or wider, within the bound.
A program may use at most 128 MiB of HBM per device.

```python
import jax
import jax.numpy as jnp
from jax import lax

D = 2048
FF = 5632
TAPS = 3
TOK_DEV = 256
TOKENS = 2048
N_FS = 8


def strengthened(entries, stream_key, source, target, shards_of, factor):
    owner, partner = [(jnp.arange(entries.shape[position]) // (entries.shape[position] // shards_of)).reshape([-1 if axis == position else 1 for axis in range(entries.ndim)]) for position in (source, target)]
    chosen = jax.random.permutation(stream_key, shards_of)[partner]
    strong = (owner == chosen) | (owner == (partner + shards_of // 2) % shards_of)
    return jnp.where(strong, factor * entries, entries)


def levels(own_key, dims, pieces, least, high):
    def one(axis_at, parts):
        steps = jax.random.uniform(jax.random.fold_in(jax.random.fold_in(own_key, 6), axis_at), (parts,), jnp.float32, least / len(pieces), high / len(pieces))
        return jnp.repeat(jnp.exp(steps), dims[axis_at] // parts).reshape((-1,) + (1,) * (len(dims) - axis_at - 1))

    level = one(*pieces[0])
    for cut in pieces[1:]:
        level = level * one(*cut)
    return level


def bell_draw(own_key, shape, spread, bound, cuts=(), dtype=jnp.bfloat16):
    gain = levels(own_key, shape, cuts, -0.22, 0.18) if cuts else 1.0
    drawn = jax.random.normal(own_key, shape, jnp.float32) * spread * gain
    return jnp.minimum(jnp.maximum(drawn, -bound), bound).astype(dtype)


def bell_draw_with(rng, extent, width, bound, pieces, heavy, held_as=jnp.bfloat16):
    drawn = width * jax.random.normal(rng, extent, jnp.float32)
    if pieces:
        drawn = drawn * levels(rng, extent, pieces, -0.22, 0.18)
    return jnp.clip(strengthened(drawn, jax.random.fold_in(rng, 3), *heavy), -bound, bound).astype(held_as)


def setup_inputs(seed: int = 0, part: int = 0) -> dict:
    key_list = jax.random.split(jax.random.key(seed), 12)
    own_keys = jax.random.split(jax.random.fold_in(key_list[11], part), 12)
    return {
        "late_rows": bell_draw(own_keys[0], (TOKENS, D), 1.0, 6.0, ((0, 8),)),
        "early_rows": bell_draw_with(own_keys[1], (TOKENS, D), 1.0, 6.0, ((0, 8),), (0, 1, 8, 2.0)),
        "hidden_cot": bell_draw_with(own_keys[2], (TOKENS, FF), 1.0, 6.0, ((0, 8), (1, 2)), (0, 1, 8, 2.0)),
        "gate_weight": bell_draw(key_list[3], (D, FF), D ** -0.5, 0.125, ((0, 8), (1, 2))),
        "up_weight": bell_draw(key_list[4], (D, FF), D ** -0.5, 0.125, ((0, 8), (1, 2))),
        "gate_taps": bell_draw(key_list[5], (TAPS, FF), TAPS ** -0.5, 3.5, ((1, 2),)),
        "up_taps": bell_draw(key_list[6], (TAPS, FF), TAPS ** -0.5, 3.5, ((1, 2),)),
        "gate_grad_sum": bell_draw(own_keys[7], (D, FF), 1.0, 6.0, ((0, 8), (1, 2)), jnp.float32),
        "up_grad_sum": bell_draw(own_keys[8], (D, FF), 1.0, 6.0, ((0, 8), (1, 2)), jnp.float32),
        "gate_taps_sum": bell_draw(own_keys[9], (TAPS, FF), 1.0, 6.0, ((1, 2),), jnp.float32),
        "up_taps_sum": bell_draw(own_keys[10], (TAPS, FF), 1.0, 6.0, ((1, 2),), jnp.float32),
    }


def causal_mix(values, filter_taps):
    length = values.shape[-2]
    widths = [(0, 0)] * values.ndim
    widths[-2] = (2, 0)
    padded = jnp.pad(values, widths)
    return filter_taps[0] * padded[..., 0:length, :] + filter_taps[1] * padded[..., 1:length + 1, :] + filter_taps[2] * padded[..., 2:length + 2, :]

def mix_back(grads, filter_taps):
    length = grads.shape[-2]
    widths = [(0, 0)] * grads.ndim
    widths[-2] = (0, 2)
    padded = jnp.pad(grads, widths)
    return filter_taps[2] * padded[..., 0:length, :] + filter_taps[1] * padded[..., 1:length + 1, :] + filter_taps[0] * padded[..., 2:length + 2, :]

def tap_products(grads, values):
    length = values.shape[-2]
    widths = [(0, 0)] * values.ndim
    widths[-2] = (2, 0)
    padded = jnp.pad(values, widths)
    axes = tuple(range(values.ndim - 1))
    return jnp.stack([lax.optimization_barrier(jnp.sum(grads * padded[..., offset:offset + length, :], axis=axes)) for offset in range(3)])

def stored(product):
    return lax.optimization_barrier(product.astype(jnp.bfloat16)).astype(jnp.float32)

def reference(late_rows, early_rows, hidden_cot, gate_weight, up_weight, gate_taps, up_taps, gate_grad_sum, up_grad_sum, gate_taps_sum, up_taps_sum):
    rows_scale = TOKENS ** (-0.5)
    gate_filter = gate_taps.astype(jnp.float32)
    up_filter = up_taps.astype(jnp.float32)

    def project(source):
        gate_pre = stored(jnp.dot(source, gate_weight, preferred_element_type=jnp.float32))
        up_pre = stored(jnp.dot(source, up_weight, preferred_element_type=jnp.float32))
        return (gate_pre.reshape(N_FS, TOK_DEV, FF), up_pre.reshape(N_FS, TOK_DEV, FF))
    late_gate, late_up = project(late_rows)
    late_hidden = (jax.nn.gelu(causal_mix(late_gate, gate_filter), approximate=True) * causal_mix(late_up, up_filter)).astype(jnp.bfloat16).reshape(TOKENS, FF)
    early_gate, early_up = project(early_rows)
    gate_mix = causal_mix(early_gate, gate_filter)
    up_mix = causal_mix(early_up, up_filter)
    cotangent = hidden_cot.astype(jnp.float32).reshape(N_FS, TOK_DEV, FF)
    activated, gelu_back = jax.vjp(lambda mixed_value: jax.nn.gelu(mixed_value, approximate=True), gate_mix)
    d_gate_mix = gelu_back(cotangent * up_mix)[0]
    d_up_mix = cotangent * activated
    d_gate_pre = mix_back(d_gate_mix, gate_filter).astype(jnp.bfloat16)
    d_up_pre = mix_back(d_up_mix, up_filter).astype(jnp.bfloat16)
    gate_taps_next = gate_taps_sum + rows_scale * tap_products(d_gate_mix, early_gate)
    up_taps_next = up_taps_sum + rows_scale * tap_products(d_up_mix, early_up)
    flat_gate = d_gate_pre.reshape(TOKENS, FF)
    flat_up = d_up_pre.reshape(TOKENS, FF)
    early_grad = (jnp.dot(flat_gate, gate_weight.T, preferred_element_type=jnp.float32) + jnp.dot(flat_up, up_weight.T, preferred_element_type=jnp.float32)).astype(jnp.bfloat16)
    both_grads = jnp.concatenate([d_gate_pre, d_up_pre], axis=-1)
    blocks = early_rows.reshape(N_FS, TOK_DEV, D)

    def add_device(total, pair):
        block_rows, block_grads = pair
        term = (jnp.dot(block_rows.T, block_grads, preferred_element_type=jnp.float32) * rows_scale).astype(jnp.bfloat16)
        term = lax.optimization_barrier(term)
        return (total + term.astype(jnp.float32), None)
    summed = lax.scan(add_device, jnp.zeros((D, 2 * FF), jnp.float32), (blocks, both_grads))[0]
    return (late_hidden, early_grad, gate_grad_sum + summed[:, :FF], up_grad_sum + summed[:, FF:], gate_taps_next, up_taps_next)
```

```python
import functools
import math

import jax
import jax.numpy as jnp
from jax import lax
from jax.experimental import pallas as pl
from jax.experimental.pallas import tpu as pltpu
from jax.sharding import PartitionSpec as P

contract_last = (((1,), (1,)), ((), ()))
contract_first = (((0,), (0,)), ((), ()))


BF, F32 = jnp.bfloat16, jnp.float32
MESH = pl.DeviceIdType.MESH
LANES = 128
ROOT = math.sqrt(2 / math.pi)
CUBIC = 0.044715


def causal_mix(values, filter_taps):
    length = values.shape[-2]
    widths = [(0, 0)] * values.ndim
    widths[-2] = (2, 0)
    padded = jnp.pad(values, widths)
    return (
        filter_taps[0] * padded[..., 0:length, :]
        + filter_taps[1] * padded[..., 1 : length + 1, :]
        + filter_taps[2] * padded[..., 2 : length + 2, :]
    )


def mix_back(grads, filter_taps):
    length = grads.shape[-2]
    widths = [(0, 0)] * grads.ndim
    widths[-2] = (0, 2)
    padded = jnp.pad(grads, widths)
    return (
        filter_taps[2] * padded[..., 0:length, :]
        + filter_taps[1] * padded[..., 1 : length + 1, :]
        + filter_taps[0] * padded[..., 2 : length + 2, :]
    )


def tap_products(grads, values):
    length = values.shape[-2]
    widths = [(0, 0)] * values.ndim
    widths[-2] = (2, 0)
    padded = jnp.pad(values, widths)
    axes = tuple(range(values.ndim - 1))
    return jnp.stack(
        [
            jnp.sum(grads * padded[..., offset : offset + length, :], axis=axes)
            for offset in range(3)
        ]
    )


def stored(product):
    return lax.optimization_barrier(product.astype(jnp.bfloat16)).astype(jnp.float32)


def per_device(
    late_rows,
    early_rows,
    hidden_cot,
    gate_weight,
    up_weight,
    gate_taps,
    up_taps,
    gate_grad_sum,
    up_grad_sum,
    gate_taps_sum,
    up_taps_sum,
):
    row_count = late_rows.shape[0]
    width_local = gate_weight.shape[1]
    rows_scale = (row_count * lax.axis_size("fs")) ** (-0.5)
    gate_filter = gate_taps.astype(jnp.float32)
    up_filter = up_taps.astype(jnp.float32)
    joined_weight = jnp.concatenate([gate_weight, up_weight], axis=1)
    both_rows = jnp.concatenate([late_rows, early_rows], axis=0)
    whole_joined = lax.all_gather(joined_weight, "fs", axis=0, tiled=True)
    projected = jnp.dot(both_rows, whole_joined, preferred_element_type=jnp.float32)
    projected = stored(projected)
    late_gate = projected[:row_count, :width_local]
    late_up = projected[:row_count, width_local:]
    early_gate = projected[row_count:, :width_local]
    early_up = projected[row_count:, width_local:]
    late_hidden = (
        jax.nn.gelu(causal_mix(late_gate, gate_filter), approximate=True)
        * causal_mix(late_up, up_filter)
    ).astype(jnp.bfloat16)
    gate_mix = causal_mix(early_gate, gate_filter)
    up_mix = causal_mix(early_up, up_filter)
    cotangent = hidden_cot.astype(jnp.float32)
    activated, gelu_back = jax.vjp(
        lambda mixed_value: jax.nn.gelu(mixed_value, approximate=True), gate_mix
    )
    d_gate_mix = gelu_back(cotangent * up_mix)[0]
    d_up_mix = cotangent * activated
    d_gate_pre = mix_back(d_gate_mix, gate_filter).astype(jnp.bfloat16)
    d_up_pre = mix_back(d_up_mix, up_filter).astype(jnp.bfloat16)
    both_grads = jnp.concatenate([d_gate_pre, d_up_pre], axis=1)
    early_grad = lax.psum(
        lax.dot_general(
            both_grads, whole_joined, contract_last, preferred_element_type=jnp.float32
        ).astype(jnp.bfloat16),
        "tp",
    )
    summed = lax.psum_scatter(
        (
            lax.dot_general(
                early_rows, both_grads, contract_first, preferred_element_type=jnp.float32
            )
            * rows_scale
        ).astype(jnp.bfloat16),
        "fs",
        scatter_dimension=0,
        tiled=True,
    ).astype(jnp.float32)
    gate_tap_sums, up_tap_sums = lax.psum(
        (
            rows_scale * tap_products(d_gate_mix, early_gate),
            rows_scale * tap_products(d_up_mix, early_up),
        ),
        "fs",
    )
    return (
        late_hidden,
        early_grad,
        gate_grad_sum + summed[:, :width_local],
        up_grad_sum + summed[:, width_local:],
        gate_taps_sum + gate_tap_sums,
        up_taps_sum + up_tap_sums,
    )


def moved_rows(values, count):
    rows = lax.broadcasted_iota(jnp.int32, values.shape, 0)
    length = values.shape[0]
    if count > 0:
        return jnp.where(rows >= count, pltpu.roll(values, count, 0), 0.0)
    return jnp.where(rows < length + count, pltpu.roll(values, length + count, 0), 0.0)


def mixed(values, taps):
    return (
        taps[0] * moved_rows(values, 2) + taps[1] * moved_rows(values, 1) + taps[2] * values
    )


def mixed_back(values, taps):
    return (
        taps[2] * values + taps[1] * moved_rows(values, -1) + taps[0] * moved_rows(values, -2)
    )


CHUNK_RECV = ("we", "ce", "wyg", "wyu", "cy", "lg", "lu", "lc", "xe", "xy", "bw", "bc", "xb")
CHUNK_SEND = ("wyg", "wyu", "cy", "we", "ce", "xe", "xy", "bw", "bc", "xb")


class Plan:
    def __init__(self, chunks):
        self.chunks = chunks
        self.recv, self.send = {}, {}
        self.recv_count = self.send_count = 0
        self.add_recv("re", 16)
        self.add_recv("rl", 8)
        for name in CHUNK_RECV:
            self.add_recv(name, chunks)
        self.add_recv("out", 6)
        self.add_recv("own", 3)
        self.add_recv("tap", 2)
        self.add_recv("owntap", 1)
        self.add_recv("gc", 2)
        self.add_recv("gy", 2)
        self.add_recv("ge", 1)
        self.add_recv("gf", 1)
        self.add_recv("gl", 1)
        for name in CHUNK_SEND:
            self.add_send(name, 1)
        self.add_send("rows", 24)
        self.add_send("out", 9)
        self.add_send("tap", 3)
        self.add_send("gc", 2)
        self.add_send("gy", 2)
        self.add_send("ge", 1)
        self.add_send("gf", 1)

    def add_recv(self, name, count):
        self.recv[name] = self.recv_count
        self.recv_count += count

    def add_send(self, name, count):
        self.send[name] = self.send_count
        self.send_count += count


def layer_kernel(
    plan,
    scale,
    late_ref,
    early_ref,
    cot_ref,
    gate_ref,
    up_ref,
    taps_ref,
    hid_ref,
    eg_ref,
    gw_ref,
    uw_ref,
    tap_ref,
    w_buf,
    c_buf,
    re_buf,
    rl_buf,
    rt_buf,
    dp_buf,
    g_buf,
    ho_buf,
    wg_buf,
    ts_buf,
    tt_buf,
    sb_buf,
    sc_buf,
    sy_buf,
    ry_buf,
    fo_buf,
    send_sems,
    recv_sems,
):
    chunks = plan.chunks
    span = chunks * LANES
    model = re_buf.shape[3]
    half_rows = re_buf.shape[2]
    seq = 2 * half_rows
    x = lax.axis_index("rep")
    fs = lax.axis_index("fs")
    c = lax.axis_index("tp")
    z = fs // 2
    y = fs % 2
    hz = z // 2
    xo, yo, co = 1 - x, 1 - y, 1 - c
    zm, ze, zo = 1 + hz, 3 * hz, 2 - hz
    zoe = 3 - ze
    is_mid = z == zm
    is_end = z == ze

    def at(zz, yy):
        return zz * 2 + yy

    def local(zz, yy):
        return (zz - 2 * hz) * 2 + yy

    def recv(name, index=0):
        return recv_sems.at[plan.recv[name] + index]

    def send(name, index=0):
        return send_sems.at[plan.send[name] + index]

    def remote(src, dst, send_sem, recv_sem, target):
        return pltpu.make_async_remote_copy(
            src_ref=src,
            dst_ref=dst,
            send_sem=send_sem,
            recv_sem=recv_sem,
            device_id=target,
            device_id_type=MESH,
        )

    partner = (x, fs, co)
    across = (x, at(z, yo), c)
    facing = (xo, fs, c)
    home = (x, at(zm, y), c)
    beyond = (x, at(zo, y), c)

    def arrived(ref, sem):
        remote(ref, ref, send("rows"), sem, partner).wait_recv()

    def sent(ref, sem):
        remote(ref, ref, sem, recv("re"), partner).wait_send()

    def copied(ref, sem):
        pltpu.make_async_copy(ref, ref, sem).wait()

    def columns(side, h):
        return pl.ds(pl.multiple_of(side * span + h * LANES, LANES), LANES)

    whole = lambda side: pl.ds(pl.multiple_of(side * span, LANES), span)
    left, right = pl.ds(0, LANES), pl.ds(LANES, LANES)
    ends = pl.ds(2 * ze, 2)
    ours = pl.ds(4 * hz, 4)
    theirs = pl.ds(4 * (1 - hz), 4)

    def gather_own(h, rows):
        pltpu.make_async_copy(
            gate_ref.at[rows, :, columns(y, h)], w_buf.at[h, fs, rows, :, left], recv("lg", h)
        ).start()
        pltpu.make_async_copy(
            up_ref.at[rows, :, columns(y, h)], w_buf.at[h, fs, rows, :, right], recv("lu", h)
        ).start()
        pltpu.make_async_copy(
            cot_ref.at[:, columns(y, h)], c_buf.at[h, fs], recv("lc", h)
        ).start()

    def own_gathered(h, rows):
        copied(w_buf.at[h, fs, rows, :, left], recv("lg", h))
        copied(w_buf.at[h, fs, rows, :, right], recv("lu", h))
        copied(c_buf.at[h, fs], recv("lc", h))

    def give_across(h):
        remote(
            gate_ref.at[x, :, columns(yo, h)],
            w_buf.at[h, fs, x, :, left],
            send("wyg"),
            recv("wyg", h),
            across,
        ).start()
        remote(
            up_ref.at[x, :, columns(yo, h)],
            w_buf.at[h, fs, x, :, right],
            send("wyu"),
            recv("wyu", h),
            across,
        ).start()
        remote(
            cot_ref.at[:, columns(yo, h)],
            c_buf.at[h, fs],
            send("cy"),
            recv("cy", h),
            across,
        ).start()

    def across_given(h):
        other = at(z, yo)
        arrived(w_buf.at[h, other, x, :, left], recv("wyg", h))
        arrived(w_buf.at[h, other, x, :, right], recv("wyu", h))
        arrived(c_buf.at[h, other], recv("cy", h))

    def across_sent():
        sent(gate_ref.at[x, :, whole(yo)], send("wyg"))
        sent(up_ref.at[x, :, whole(yo)], send("wyu"))
        sent(cot_ref.at[:, whole(yo)], send("cy"))

    def early_copy(src, f, half, number, target):
        return remote(
            src, re_buf.at[f, half], send("rows", number), recv("re", f * 2 + half), target
        )

    def late_copy(src, fl, half, number, target):
        return remote(
            src, rl_buf.at[fl, half], send("rows", number), recv("rl", fl * 2 + half), target
        )

    def early_here(f, half):
        arrived(re_buf.at[f, half], recv("re", f * 2 + half))

    def late_here(fl, half):
        arrived(rl_buf.at[fl, half], recv("rl", fl * 2 + half))

    @pl.when(is_end)
    def _():
        mine, other = at(ze, y), at(ze, yo)
        mine_l, other_l = local(ze, y), local(ze, yo)
        early_copy(early_ref.at[c], mine, c, 0, home).start()
        early_copy(early_ref.at[c], mine, c, 1, across).start()
        give_across(0)
        late_copy(late_ref.at[c], mine_l, c, 2, across).start()

        def give(h, _):
            give_across(h)
            return 0

        lax.fori_loop(1, chunks, give, 0)

        def own(h, _):
            gather_own(h, x)
            return 0

        lax.fori_loop(0, chunks, own, 0)

        early_here(other, c)
        early_copy(re_buf.at[other, c], other, c, 3, home).start()

        def hand_on(h):
            own_gathered(h, x)
            across_given(h)
            remote(
                w_buf.at[h, ends, x], w_buf.at[h, ends, x], send("we"), recv("we", h), home
            ).start()
            remote(
                c_buf.at[h, ends], c_buf.at[h, ends], send("ce"), recv("ce", h), home
            ).start()

        hand_on(0)
        late_copy(late_ref.at[c], mine_l, c, 4, home).start()
        late_here(other_l, c)
        late_copy(rl_buf.at[other_l, c], other_l, c, 5, home).start()

        def each(h, _):
            hand_on(h)
            return 0

        lax.fori_loop(1, chunks, each, 0)

        sent(early_ref.at[c], send("rows", 0))
        sent(early_ref.at[c], send("rows", 1))
        sent(late_ref.at[c], send("rows", 2))
        sent(early_ref.at[c], send("rows", 3))
        sent(late_ref.at[c], send("rows", 4))
        sent(late_ref.at[c], send("rows", 5))
        across_sent()
        sent(w_buf.at[:, ends, x], send("we"))
        sent(c_buf.at[:, ends], send("ce"))

        arrived(fo_buf.at[0], recv("ge"))
        remote(fo_buf.at[0], eg_ref.at[c], send("gf"), recv("gf"), partner).start()
        keep = pltpu.make_async_copy(fo_buf.at[0], eg_ref.at[c], recv("gl"))
        keep.start()
        keep.wait()
        sent(fo_buf.at[0], send("gf"))
        arrived(eg_ref.at[co], recv("gf"))

        for side in range(2):
            arrived(hid_ref.at[:, pl.ds(side * span, span)], recv("out", side * 3))
            arrived(gw_ref.at[:, pl.ds(side * span, span)], recv("out", side * 3 + 1))
            arrived(uw_ref.at[:, pl.ds(side * span, span)], recv("out", side * 3 + 2))
            arrived(tap_ref.at[side], recv("tap", side))

    @pl.when(is_mid)
    def _():
        mine, other = at(zm, y), at(zm, yo)
        mine_l, other_l = local(zm, y), local(zm, yo)
        both = pl.ds(0, 2)

        keep_early = pltpu.make_async_copy(early_ref, re_buf.at[mine], recv("re", mine * 2))
        keep_late = pltpu.make_async_copy(late_ref, rl_buf.at[mine_l], recv("rl", mine_l * 2))
        keep_early.start()
        keep_late.start()
        early_copy(early_ref.at[c], mine, c, 0, beyond).start()
        give_across(0)
        early_copy(early_ref.at[c], mine, c, 1, across).start()

        def own(h, _):
            gather_own(h, both)
            return 0

        lax.fori_loop(0, chunks, own, 0)
        g_buf[...] = jnp.zeros_like(g_buf)

        def turn(f):
            def one(fl, _):
                cols = pl.ds(pl.multiple_of((4 * hz + fl) * seq, LANES), seq)
                block = re_buf[f, :, :, cols].reshape(seq, seq)
                rt_buf[fl, :, pl.ds(pl.multiple_of(f * seq, LANES), seq)] = block.T
                return 0

            lax.fori_loop(0, 4, one, 0)

        def swap_early(f, number):
            early_copy(re_buf.at[f, c], f, c, number, partner).start()

        def swap_late(fl, number):
            late_copy(rl_buf.at[fl, c], fl, c, number, partner).start()

        def pass_on(h):
            own_gathered(h, both)
            across_given(h)
            arrived(w_buf.at[h, ends, x], recv("we", h))
            remote(
                w_buf.at[h, ours, x], w_buf.at[h, ours, x], send("bw"), recv("bw", h), beyond
            ).start()
            remote(
                w_buf.at[h, ends, x], w_buf.at[h, ends, x], send("xe"), recv("xe", h), facing
            ).start()
            remote(
                w_buf.at[h, other, x], w_buf.at[h, other, x], send("xy"), recv("xy", h), facing
            ).start()
            arrived(c_buf.at[h, ends], recv("ce", h))
            remote(
                c_buf.at[h, ours], c_buf.at[h, ours], send("bc"), recv("bc", h), beyond
            ).start()

        def pass_over(h):
            arrived(w_buf.at[h, theirs, x], recv("bw", h))
            remote(
                w_buf.at[h, theirs, x], w_buf.at[h, theirs, x], send("xb"), recv("xb", h), facing
            ).start()

        def complete(h):
            arrived(w_buf.at[h, ends, xo], recv("xe", h))
            arrived(w_buf.at[h, other, xo], recv("xy", h))
            arrived(w_buf.at[h, theirs, xo], recv("xb", h))
            arrived(c_buf.at[h, theirs], recv("bc", h))

        near, far = at(zo, y), at(zoe, y)
        near_o, far_o = at(zo, yo), at(zoe, yo)
        end_y, end_o = at(ze, y), at(ze, yo)

        early_here(end_y, c)
        early_copy(re_buf.at[end_y, c], end_y, c, 2, beyond).start()
        swap_early(end_y, 3)
        early_here(end_o, c)
        swap_early(end_o, 4)
        early_here(other, c)
        swap_early(other, 5)
        pass_on(0)
        keep_early.wait()
        turn(mine)
        early_here(near, c)
        early_copy(re_buf.at[near, c], near, c, 6, across).start()
        swap_early(near, 7)
        for f in (end_y, end_o, other):
            early_here(f, co)
            turn(f)
        early_here(far, c)
        early_copy(re_buf.at[far, c], far, c, 8, across).start()
        swap_early(far, 9)
        give_across(1)
        late_copy(late_ref.at[c], mine_l, c, 12, across).start()

        def give(h, _):
            give_across(h)
            return 0

        lax.fori_loop(2, chunks, give, 0)
        early_here(near, co)
        turn(near)
        early_here(near_o, c)
        swap_early(near_o, 10)
        pass_on(1)
        pass_over(0)
        early_here(far, co)
        turn(far)
        early_here(far_o, c)
        swap_early(far_o, 11)
        for fl, number in ((local(ze, y), 13), (local(ze, yo), 14), (other_l, 15)):
            late_here(fl, c)
            swap_late(fl, number)
        for f in (near_o, far_o):
            early_here(f, co)
            turn(f)
        keep_late.wait()
        for fl in (local(ze, y), local(ze, yo), other_l):
            late_here(fl, co)
        pass_on(2)

        def chunk(h, _):
            complete(h)

            @pl.when(h + 1 < chunks)
            def _():
                pass_over(h + 1)

            @pl.when(h + 3 < chunks)
            def _():
                pass_on(h + 3)

            cols = columns(y, h)
            gate_taps = [taps_ref[j : j + 1, cols] for j in range(3)]
            up_taps = [taps_ref[j + 3 : j + 4, cols] for j in range(3)]

            def weight():
                return w_buf[h].reshape(model, 2 * LANES)

            ts_buf[...] = jnp.zeros_like(ts_buf)

            def early(f, group):
                pre = jnp.dot(
                    re_buf[f].reshape(seq, model), weight(), preferred_element_type=F32
                ).astype(BF)
                gate_pre = pre[:, :LANES].astype(F32)
                up_pre = pre[:, LANES:].astype(F32)
                gate_mix = mixed(gate_pre, gate_taps)
                up_mix = mixed(up_pre, up_taps)
                cot = c_buf[h, f].astype(F32)
                square = gate_mix * gate_mix
                tanh = jnp.tanh(ROOT * gate_mix * (1.0 + CUBIC * square))
                half = 0.5 * (1.0 + tanh)
                slope = half + 0.5 * gate_mix * (1.0 - tanh * tanh) * (
                    ROOT * (1.0 + 3 * CUBIC * square)
                )
                d_gate = cot * up_mix * slope
                d_up = cot * (gate_mix * half)
                sums = []
                for grad, value in ((d_gate, gate_pre), (d_up, up_pre)):
                    for j in range(3):
                        other_value = moved_rows(value, 2 - j) if j < 2 else value
                        product = grad * other_value
                        sums.append(product.reshape(seq // 8, 8, LANES).sum(0))
                ts_buf[group] += jnp.stack(sums)
                back = jnp.concatenate(
                    [
                        mixed_back(d_gate, gate_taps).astype(BF),
                        mixed_back(d_up, up_taps).astype(BF),
                    ],
                    axis=1,
                )
                dp_buf[f] = back
                return back

            def own_early(fl, _):
                back = early(4 * hz + fl, hz)
                term = lax.dot_general(
                    back, weight(), contract_last, preferred_element_type=F32
                )
                g_buf[fl] += term.reshape(2, half_rows, model)
                return 0

            lax.fori_loop(0, 4, own_early, 0)

            def other_early(fl, _):
                early(4 * (1 - hz) + fl, 1 - hz)
                return 0

            lax.fori_loop(0, 4, other_early, 0)

            def late(fl, _):
                pre = jnp.dot(
                    rl_buf[fl].reshape(seq, model), weight(), preferred_element_type=F32
                ).astype(BF)
                gate_mix = mixed(pre[:, :LANES].astype(F32), gate_taps)
                up_mix = mixed(pre[:, LANES:].astype(F32), up_taps)
                tanh = jnp.tanh(ROOT * gate_mix * (1.0 + CUBIC * gate_mix * gate_mix))
                ho_buf[h, fl] = (0.5 * gate_mix * (1.0 + tanh) * up_mix).astype(BF)
                return 0

            lax.fori_loop(0, 4, late, 0)

            def weight_grad(fl, _):
                product = jnp.dot(
                    rt_buf[fl],
                    dp_buf[...].reshape(8 * seq, 2 * LANES),
                    preferred_element_type=F32,
                )
                wg_buf[h, fl] = (product * scale).astype(BF)
                return 0

            lax.fori_loop(0, 4, weight_grad, 0)
            total = ts_buf[0] + ts_buf[1]
            here = pl.ds(pl.multiple_of(h * LANES, LANES), LANES)
            tt_buf[pl.ds(0, 6), here] = jnp.sum(total, axis=1)

            for number, (zz, yy) in enumerate(((ze, y), (ze, yo), (zm, yo))):
                fl = local(zz, yy)
                target = (x, at(zz, yy), c)
                for kind, (src, dst) in enumerate(
                    (
                        (ho_buf.at[h, fl], hid_ref),
                        (wg_buf.at[h, fl, :, left], gw_ref),
                        (wg_buf.at[h, fl, :, right], uw_ref),
                    )
                ):
                    remote(
                        src,
                        dst.at[:, cols],
                        send("out", number * 3 + kind),
                        recv("out", y * 3 + kind),
                        target,
                    ).start()
            for kind, (src, dst) in enumerate(
                (
                    (ho_buf.at[h, mine_l], hid_ref),
                    (wg_buf.at[h, mine_l, :, left], gw_ref),
                    (wg_buf.at[h, mine_l, :, right], uw_ref),
                )
            ):
                pltpu.make_async_copy(src, dst.at[:, cols], recv("own", kind)).start()
            return 0

        lax.fori_loop(0, chunks, chunk, 0)

        block = 16

        def by_rows(step):
            def one(i, _):
                step(pl.ds(pl.multiple_of(i * block, block), block))
                return 0

            lax.fori_loop(0, half_rows // block, one, 0)

        def base(p):
            return 2 * hz if p == 0 else 2 * (1 - hz)

        for p in range(2):

            def narrow(rows, p=p):
                for side in range(2):
                    sb_buf[2 * p + side, rows] = g_buf[base(p) + side, co, rows].astype(BF)

            by_rows(narrow)
            pair = pl.ds(2 * p, 2)
            remote(
                sb_buf.at[pair], sc_buf.at[pair], send("gc", p), recv("gc", p), partner
            ).start()
        for number, (zz, yy) in enumerate(((ze, y), (ze, yo), (zm, yo))):
            remote(
                tt_buf,
                tap_ref.at[y],
                send("tap", number),
                recv("tap", y),
                (x, at(zz, yy), c),
            ).start()
        pltpu.make_async_copy(tt_buf, tap_ref.at[y], recv("owntap")).start()
        for p in range(2):
            pair = pl.ds(2 * p, 2)
            arrived(sc_buf.at[pair], recv("gc", p))

            def first(rows, p=p):
                sy_buf[p, rows] = (
                    g_buf[base(p) + yo, c, rows] + sc_buf[2 * p + yo, rows].astype(F32)
                ).astype(BF)

            by_rows(first)
            remote(sy_buf.at[p], ry_buf.at[p], send("gy", p), recv("gy", p), across).start()
        for p in range(2):
            arrived(ry_buf.at[p], recv("gy", p))

            def second(rows, p=p):
                fo_buf[p, rows] = (
                    g_buf[base(p) + y, c, rows]
                    + sc_buf[2 * p + y, rows].astype(F32)
                    + ry_buf[p, rows].astype(F32)
                ).astype(BF)

            by_rows(second)
            if p == 0:
                remote(
                    fo_buf.at[0],
                    fo_buf.at[0],
                    send("ge"),
                    recv("ge"),
                    (x, at(ze, y), c),
                ).start()
            else:
                remote(fo_buf.at[1], eg_ref.at[c], send("gf"), recv("gf"), partner).start()
                pltpu.make_async_copy(fo_buf.at[1], eg_ref.at[c], recv("gl")).start()

        for number in range(16):
            sent(early_ref.at[c], send("rows", number))
        across_sent()
        sent(w_buf.at[:, ours, x], send("bw"))
        sent(w_buf.at[:, ends, x], send("xe"))
        sent(w_buf.at[:, other, x], send("xy"))
        sent(w_buf.at[:, theirs, x], send("xb"))
        sent(c_buf.at[:, ours], send("bc"))
        for number, (zz, yy) in enumerate(((ze, y), (ze, yo), (zm, yo))):
            fl = local(zz, yy)
            sent(ho_buf.at[:, fl], send("out", number * 3))
            sent(wg_buf.at[:, fl, :, left], send("out", number * 3 + 1))
            sent(wg_buf.at[:, fl, :, right], send("out", number * 3 + 2))
            sent(tt_buf, send("tap", number))
        for p in range(2):
            sent(sb_buf.at[pl.ds(2 * p, 2)], send("gc", p))
            sent(sy_buf.at[p], send("gy", p))
        sent(fo_buf.at[0], send("ge"))
        sent(fo_buf.at[1], send("gf"))
        copied(eg_ref.at[c], recv("gl"))
        arrived(eg_ref.at[co], recv("gf"))
        for kind, ref in enumerate((hid_ref, gw_ref, uw_ref)):
            copied(ref.at[:, whole(y)], recv("own", kind))
            arrived(ref.at[:, whole(yo)], recv("out", yo * 3 + kind))
        copied(tap_ref.at[y], recv("owntap"))
        arrived(tap_ref.at[yo], recv("tap", yo))


def by_halves(
    late_rows,
    early_rows,
    hidden_cot,
    gate_weight,
    up_weight,
    gate_taps,
    up_taps,
    gate_grad_sum,
    up_grad_sum,
    gate_taps_sum,
    up_taps_sum,
):
    fs_size = lax.axis_size("fs")
    rows, model = late_rows.shape
    width = gate_weight.shape[1]
    span = width // 2
    chunks = span // LANES
    half_rows = rows // 2
    scale = (rows * fs_size) ** (-0.5)
    plan = Plan(chunks)
    taps = jnp.concatenate([gate_taps, up_taps], axis=0).astype(F32)
    anywhere = pl.BlockSpec(memory_space=pl.ANY)
    vmem = pltpu.VMEM
    hidden, grad, gate_sum, up_sum, tap_sum = pl.pallas_call(
        functools.partial(layer_kernel, plan, scale),
        out_shape=(
            jax.ShapeDtypeStruct((rows, width), BF),
            jax.ShapeDtypeStruct((2, half_rows, model), BF),
            jax.ShapeDtypeStruct((rows, width), BF),
            jax.ShapeDtypeStruct((rows, width), BF),
            jax.ShapeDtypeStruct((2, 8, span), F32),
        ),
        in_specs=[anywhere] * 5 + [pl.BlockSpec(memory_space=vmem)],
        out_specs=(anywhere,) * 5,
        scratch_shapes=[
            vmem((chunks, fs_size, 2, half_rows, 2 * LANES), BF),
            vmem((chunks, fs_size, rows, LANES), BF),
            vmem((fs_size, 2, half_rows, model), BF),
            vmem((fs_size // 2, 2, half_rows, model), BF),
            vmem((fs_size // 2, rows, fs_size * rows), BF),
            vmem((fs_size, rows, 2 * LANES), BF),
            vmem((fs_size // 2, 2, half_rows, model), F32),
            vmem((chunks, fs_size // 2, rows, LANES), BF),
            vmem((chunks, fs_size // 2, rows, 2 * LANES), BF),
            vmem((2, 6, 8, LANES), F32),
            vmem((8, span), F32),
            vmem((4, half_rows, model), BF),
            vmem((4, half_rows, model), BF),
            vmem((2, half_rows, model), BF),
            vmem((2, half_rows, model), BF),
            vmem((2, half_rows, model), BF),
            pltpu.SemaphoreType.DMA((plan.send_count,)),
            pltpu.SemaphoreType.DMA((plan.recv_count,)),
        ],
        compiler_params=pltpu.CompilerParams(
            has_side_effects=True, vmem_limit_bytes=67043328
        ),
    )(
        late_rows.reshape(2, half_rows, model),
        early_rows.reshape(2, half_rows, model),
        hidden_cot,
        gate_weight.reshape(2, half_rows, width),
        up_weight.reshape(2, half_rows, width),
        taps,
    )
    tap_sum = scale * jnp.concatenate([tap_sum[0, :6], tap_sum[1, :6]], axis=1)
    return (
        hidden,
        grad.reshape(rows, model),
        gate_grad_sum + gate_sum.astype(F32),
        up_grad_sum + up_sum.astype(F32),
        gate_taps_sum + tap_sum[:3],
        up_taps_sum + tap_sum[3:],
    )


def solution(mesh):
    in_specs = (
        P(("rep", "fs"), None),
        P(("rep", "fs"), None),
        P(("rep", "fs"), "tp"),
        P("fs", "tp"),
        P("fs", "tp"),
        P(None, "tp"),
        P(None, "tp"),
        P(("rep", "fs"), "tp"),
        P(("rep", "fs"), "tp"),
        P("rep", "tp"),
        P("rep", "tp"),
    )
    out_specs = (
        P(("rep", "fs"), "tp"),
        P(("rep", "fs"), None),
        P(("rep", "fs"), "tp"),
        P(("rep", "fs"), "tp"),
        P("rep", "tp"),
        P("rep", "tp"),
    )
    sizes = dict(mesh.shape)

    def run(*args):
        rows = args[0].shape[0] // (sizes["rep"] * sizes["fs"])
        model = args[0].shape[1]
        width = args[3].shape[1] // sizes["tp"]
        small = rows <= 256 and model <= 2048 and width <= 2816
        even = rows % 256 == 0 and width % (2 * LANES) == 0 and model == 8 * rows
        fits = (sizes["rep"], sizes["fs"], sizes["tp"]) == (2, 8, 2) and small and even
        return jax.shard_map(
            by_halves if fits else per_device,
            mesh=mesh,
            in_specs=in_specs,
            out_specs=out_specs,
            check_vma=False,
        )(*args)

    return run
```

```python
import functools
import math

import jax
import jax.numpy as jnp
from jax import lax
from jax.experimental import pallas as pl
from jax.experimental.pallas import tpu as pltpu
from jax.sharding import PartitionSpec as P

contract_last = (((1,), (1,)), ((), ()))
contract_first = (((0,), (0,)), ((), ()))


BF, F32 = jnp.bfloat16, jnp.float32
MESH = pl.DeviceIdType.MESH
LANES = 128
ROOT = math.sqrt(2 / math.pi)
CUBIC = 0.044715


def causal_mix(values, filter_taps):
    length = values.shape[-2]
    widths = [(0, 0)] * values.ndim
    widths[-2] = (2, 0)
    padded = jnp.pad(values, widths)
    return (
        filter_taps[0] * padded[..., 0:length, :]
        + filter_taps[1] * padded[..., 1 : length + 1, :]
        + filter_taps[2] * padded[..., 2 : length + 2, :]
    )


def mix_back(grads, filter_taps):
    length = grads.shape[-2]
    widths = [(0, 0)] * grads.ndim
    widths[-2] = (0, 2)
    padded = jnp.pad(grads, widths)
    return (
        filter_taps[2] * padded[..., 0:length, :]
        + filter_taps[1] * padded[..., 1 : length + 1, :]
        + filter_taps[0] * padded[..., 2 : length + 2, :]
    )


def tap_products(grads, values):
    length = values.shape[-2]
    widths = [(0, 0)] * values.ndim
    widths[-2] = (2, 0)
    padded = jnp.pad(values, widths)
    axes = tuple(range(values.ndim - 1))
    return jnp.stack(
        [
            jnp.sum(grads * padded[..., offset : offset + length, :], axis=axes)
            for offset in range(3)
        ]
    )


def stored(product):
    return lax.optimization_barrier(product.astype(jnp.bfloat16)).astype(jnp.float32)


def per_device(
    late_rows,
    early_rows,
    hidden_cot,
    gate_weight,
    up_weight,
    gate_taps,
    up_taps,
    gate_grad_sum,
    up_grad_sum,
    gate_taps_sum,
    up_taps_sum,
):
    row_count = late_rows.shape[0]
    width_local = gate_weight.shape[1]
    rows_scale = (row_count * lax.axis_size("fs")) ** (-0.5)
    gate_filter = gate_taps.astype(jnp.float32)
    up_filter = up_taps.astype(jnp.float32)
    joined_weight = jnp.concatenate([gate_weight, up_weight], axis=1)
    both_rows = jnp.concatenate([late_rows, early_rows], axis=0)
    whole_joined = lax.all_gather(joined_weight, "fs", axis=0, tiled=True)
    projected = jnp.dot(both_rows, whole_joined, preferred_element_type=jnp.float32)
    projected = stored(projected)
    late_gate = projected[:row_count, :width_local]
    late_up = projected[:row_count, width_local:]
    early_gate = projected[row_count:, :width_local]
    early_up = projected[row_count:, width_local:]
    late_hidden = (
        jax.nn.gelu(causal_mix(late_gate, gate_filter), approximate=True)
        * causal_mix(late_up, up_filter)
    ).astype(jnp.bfloat16)
    gate_mix = causal_mix(early_gate, gate_filter)
    up_mix = causal_mix(early_up, up_filter)
    cotangent = hidden_cot.astype(jnp.float32)
    activated, gelu_back = jax.vjp(
        lambda mixed_value: jax.nn.gelu(mixed_value, approximate=True), gate_mix
    )
    d_gate_mix = gelu_back(cotangent * up_mix)[0]
    d_up_mix = cotangent * activated
    d_gate_pre = mix_back(d_gate_mix, gate_filter).astype(jnp.bfloat16)
    d_up_pre = mix_back(d_up_mix, up_filter).astype(jnp.bfloat16)
    both_grads = jnp.concatenate([d_gate_pre, d_up_pre], axis=1)
    early_grad = lax.psum(
        lax.dot_general(
            both_grads, whole_joined, contract_last, preferred_element_type=jnp.float32
        ).astype(jnp.bfloat16),
        "tp",
    )
    summed = lax.psum_scatter(
        (
            lax.dot_general(
                early_rows, both_grads, contract_first, preferred_element_type=jnp.float32
            )
            * rows_scale
        ).astype(jnp.bfloat16),
        "fs",
        scatter_dimension=0,
        tiled=True,
    ).astype(jnp.float32)
    gate_tap_sums, up_tap_sums = lax.psum(
        (
            rows_scale * tap_products(d_gate_mix, early_gate),
            rows_scale * tap_products(d_up_mix, early_up),
        ),
        "fs",
    )
    return (
        late_hidden,
        early_grad,
        gate_grad_sum + summed[:, :width_local],
        up_grad_sum + summed[:, width_local:],
        gate_taps_sum + gate_tap_sums,
        up_taps_sum + up_tap_sums,
    )


def moved_rows(values, count):
    rows = lax.broadcasted_iota(jnp.int32, values.shape, 0)
    length = values.shape[0]
    if count > 0:
        return jnp.where(rows >= count, pltpu.roll(values, count, 0), 0.0)
    return jnp.where(rows < length + count, pltpu.roll(values, length + count, 0), 0.0)


def mixed(values, taps):
    return (
        taps[0] * moved_rows(values, 2) + taps[1] * moved_rows(values, 1) + taps[2] * values
    )


def mixed_back(values, taps):
    return (
        taps[2] * values + taps[1] * moved_rows(values, -1) + taps[0] * moved_rows(values, -2)
    )


CHUNK_RECV = ("we", "ce", "wyg", "wyu", "cy", "lg", "lu", "lc", "xe", "xy", "bw", "bc", "xb")
CHUNK_SEND = ("wyg", "wyu", "cy", "we", "ce", "xe", "xy", "bw", "bc", "xb")


class Plan:
    def __init__(self, chunks):
        self.chunks = chunks
        self.recv, self.send = {}, {}
        self.recv_count = self.send_count = 0
        self.add_recv("re", 16)
        self.add_recv("rl", 8)
        for name in CHUNK_RECV:
            self.add_recv(name, chunks)
        self.add_recv("out", 6)
        self.add_recv("own", 3)
        self.add_recv("tap", 2)
        self.add_recv("owntap", 1)
        self.add_recv("gc", 2)
        self.add_recv("gy", 2)
        self.add_recv("ge", 1)
        self.add_recv("gf", 1)
        self.add_recv("gl", 1)
        for name in CHUNK_SEND:
            self.add_send(name, 1)
        self.add_send("rows", 24)
        self.add_send("out", 9)
        self.add_send("tap", 3)
        self.add_send("gc", 2)
        self.add_send("gy", 2)
        self.add_send("ge", 1)
        self.add_send("gf", 1)

    def add_recv(self, name, count):
        self.recv[name] = self.recv_count
        self.recv_count += count

    def add_send(self, name, count):
        self.send[name] = self.send_count
        self.send_count += count


def layer_kernel(
    plan,
    scale,
    late_ref,
    early_ref,
    cot_ref,
    gate_ref,
    up_ref,
    taps_ref,
    hid_ref,
    eg_ref,
    gw_ref,
    uw_ref,
    tap_ref,
    w_buf,
    c_buf,
    re_buf,
    rl_buf,
    rt_buf,
    dp_buf,
    g_buf,
    ho_buf,
    wg_buf,
    ts_buf,
    tt_buf,
    pre_a,
    pre_b,
    sb_buf,
    sc_buf,
    sy_buf,
    ry_buf,
    fo_buf,
    send_sems,
    recv_sems,
):
    chunks = plan.chunks
    span = chunks * LANES
    model = re_buf.shape[3]
    half_rows = re_buf.shape[2]
    seq = 2 * half_rows
    x = lax.axis_index("rep")
    fs = lax.axis_index("fs")
    c = lax.axis_index("tp")
    z = fs // 2
    y = fs % 2
    hz = z // 2
    xo, yo, co = 1 - x, 1 - y, 1 - c
    zm, ze, zo = 1 + hz, 3 * hz, 2 - hz
    zoe = 3 - ze
    is_mid = z == zm
    is_end = z == ze

    def at(zz, yy):
        return zz * 2 + yy

    def local(zz, yy):
        return (zz - 2 * hz) * 2 + yy

    def recv(name, index=0):
        return recv_sems.at[plan.recv[name] + index]

    def send(name, index=0):
        return send_sems.at[plan.send[name] + index]

    def remote(src, dst, send_sem, recv_sem, target):
        return pltpu.make_async_remote_copy(
            src_ref=src,
            dst_ref=dst,
            send_sem=send_sem,
            recv_sem=recv_sem,
            device_id=target,
            device_id_type=MESH,
        )

    partner = (x, fs, co)
    across = (x, at(z, yo), c)
    facing = (xo, fs, c)
    home = (x, at(zm, y), c)
    beyond = (x, at(zo, y), c)

    def arrived(ref, sem):
        remote(ref, ref, send("rows"), sem, partner).wait_recv()

    def sent(ref, sem):
        remote(ref, ref, sem, recv("re"), partner).wait_send()

    def copied(ref, sem):
        pltpu.make_async_copy(ref, ref, sem).wait()

    def columns(side, h):
        return pl.ds(pl.multiple_of(side * span + h * LANES, LANES), LANES)

    whole = lambda side: pl.ds(pl.multiple_of(side * span, LANES), span)
    left, right = pl.ds(0, LANES), pl.ds(LANES, LANES)
    ends = pl.ds(2 * ze, 2)
    ours = pl.ds(4 * hz, 4)
    theirs = pl.ds(4 * (1 - hz), 4)

    def gather_own(h, rows):
        pltpu.make_async_copy(
            gate_ref.at[rows, :, columns(y, h)], w_buf.at[h, fs, rows, :, left], recv("lg", h)
        ).start()
        pltpu.make_async_copy(
            up_ref.at[rows, :, columns(y, h)], w_buf.at[h, fs, rows, :, right], recv("lu", h)
        ).start()
        pltpu.make_async_copy(
            cot_ref.at[:, columns(y, h)], c_buf.at[h, fs], recv("lc", h)
        ).start()

    def own_weights(h, rows):
        copied(w_buf.at[h, fs, rows, :, left], recv("lg", h))
        copied(w_buf.at[h, fs, rows, :, right], recv("lu", h))

    def own_cotangent(h):
        copied(c_buf.at[h, fs], recv("lc", h))

    def give_across(h):
        remote(
            gate_ref.at[x, :, columns(yo, h)],
            w_buf.at[h, fs, x, :, left],
            send("wyg"),
            recv("wyg", h),
            across,
        ).start()
        remote(
            up_ref.at[x, :, columns(yo, h)],
            w_buf.at[h, fs, x, :, right],
            send("wyu"),
            recv("wyu", h),
            across,
        ).start()
        remote(
            cot_ref.at[:, columns(yo, h)],
            c_buf.at[h, fs],
            send("cy"),
            recv("cy", h),
            across,
        ).start()

    def across_weights(h):
        other = at(z, yo)
        arrived(w_buf.at[h, other, x, :, left], recv("wyg", h))
        arrived(w_buf.at[h, other, x, :, right], recv("wyu", h))

    def across_cotangent(h):
        arrived(c_buf.at[h, at(z, yo)], recv("cy", h))

    def give_some(first, last):
        def one(h, _):
            give_across(h)
            return 0

        lax.fori_loop(first, last, one, 0)

    def across_sent():
        sent(gate_ref.at[x, :, whole(yo)], send("wyg"))
        sent(up_ref.at[x, :, whole(yo)], send("wyu"))
        sent(cot_ref.at[:, whole(yo)], send("cy"))

    def early_copy(src, f, half, number, target):
        return remote(
            src, re_buf.at[f, half], send("rows", number), recv("re", f * 2 + half), target
        )

    def late_copy(src, fl, half, number, target):
        return remote(
            src, rl_buf.at[fl, half], send("rows", number), recv("rl", fl * 2 + half), target
        )

    def early_here(f, half):
        arrived(re_buf.at[f, half], recv("re", f * 2 + half))

    def late_here(fl, half):
        arrived(rl_buf.at[fl, half], recv("rl", fl * 2 + half))

    @pl.when(is_end)
    def _():
        mine, other = at(ze, y), at(ze, yo)
        mine_l, other_l = local(ze, y), local(ze, yo)

        def own(h, _):
            gather_own(h, x)
            return 0

        def hand_weights(h):
            own_weights(h, x)
            across_weights(h)
            remote(
                w_buf.at[h, ends, x], w_buf.at[h, ends, x], send("we"), recv("we", h), home
            ).start()

        def hand_cotangent(h):
            own_cotangent(h)
            across_cotangent(h)
            remote(
                c_buf.at[h, ends], c_buf.at[h, ends], send("ce"), recv("ce", h), home
            ).start()

        give_across(0)
        gather_own(0, x)
        give_some(1, 3)
        early_copy(early_ref.at[c], mine, c, 1, across).start()
        give_some(3, 6)
        late_copy(late_ref.at[c], mine_l, c, 2, across).start()
        give_some(6, chunks)
        lax.fori_loop(1, chunks, own, 0)

        for h in range(3):
            hand_weights(h)
        early_copy(early_ref.at[c], mine, c, 0, home).start()
        early_here(other, c)
        early_copy(re_buf.at[other, c], other, c, 3, home).start()
        for h in range(3, 6):
            hand_weights(h)
            hand_cotangent(h - 3)
        late_copy(late_ref.at[c], mine_l, c, 4, home).start()
        for h in range(6, 8):
            hand_weights(h)
            hand_cotangent(h - 3)
        late_here(other_l, c)
        late_copy(rl_buf.at[other_l, c], other_l, c, 5, home).start()

        def each(h, _):
            hand_weights(h)
            hand_cotangent(h - 3)
            return 0

        lax.fori_loop(8, chunks, each, 0)
        for h in range(chunks - 3, chunks):
            hand_cotangent(h)

        sent(early_ref.at[c], send("rows", 0))
        sent(early_ref.at[c], send("rows", 1))
        sent(late_ref.at[c], send("rows", 2))
        sent(early_ref.at[c], send("rows", 3))
        sent(late_ref.at[c], send("rows", 4))
        sent(late_ref.at[c], send("rows", 5))
        across_sent()
        sent(w_buf.at[:, ends, x], send("we"))
        sent(c_buf.at[:, ends], send("ce"))

        arrived(fo_buf.at[0], recv("ge"))
        remote(fo_buf.at[0], eg_ref.at[c], send("gf"), recv("gf"), partner).start()
        keep = pltpu.make_async_copy(fo_buf.at[0], eg_ref.at[c], recv("gl"))
        keep.start()
        keep.wait()
        sent(fo_buf.at[0], send("gf"))
        arrived(eg_ref.at[co], recv("gf"))

        for side in range(2):
            arrived(hid_ref.at[:, pl.ds(side * span, span)], recv("out", side * 3))
            arrived(gw_ref.at[:, pl.ds(side * span, span)], recv("out", side * 3 + 1))
            arrived(uw_ref.at[:, pl.ds(side * span, span)], recv("out", side * 3 + 2))
            arrived(tap_ref.at[side], recv("tap", side))

    @pl.when(is_mid)
    def _():
        mine, other = at(zm, y), at(zm, yo)
        mine_l, other_l = local(zm, y), local(zm, yo)
        both = pl.ds(0, 2)

        give_across(0)
        early_copy(early_ref.at[c], mine, c, 0, beyond).start()
        early_copy(early_ref.at[c], mine, c, 1, across).start()
        give_some(1, 3)
        gather_own(0, both)
        keep_early = pltpu.make_async_copy(early_ref, re_buf.at[mine], recv("re", mine * 2))
        keep_late = pltpu.make_async_copy(late_ref, rl_buf.at[mine_l], recv("rl", mine_l * 2))
        keep_early.start()

        def own(h, _):
            gather_own(h, both)
            return 0

        lax.fori_loop(1, chunks, own, 0)
        keep_late.start()

        def clear(fl, _):
            g_buf[fl] = jnp.zeros_like(g_buf[0])
            return 0

        lax.fori_loop(0, 4, clear, 0)

        def turn(f):
            def one(fl, _):
                cols = pl.ds(pl.multiple_of((4 * hz + fl) * seq, LANES), seq)
                block = re_buf[f, :, :, cols].reshape(seq, seq)
                rt_buf[fl, :, pl.ds(pl.multiple_of(f * seq, LANES), seq)] = block.T
                return 0

            lax.fori_loop(0, 4, one, 0)

        def swap_early(f, number):
            early_copy(re_buf.at[f, c], f, c, number, partner).start()

        def swap_late(fl, number):
            late_copy(rl_buf.at[fl, c], fl, c, number, partner).start()

        def pass_weights(h):
            own_weights(h, both)
            across_weights(h)
            arrived(w_buf.at[h, ends, x], recv("we", h))
            remote(
                w_buf.at[h, ours, x], w_buf.at[h, ours, x], send("bw"), recv("bw", h), beyond
            ).start()
            remote(
                w_buf.at[h, ends, x], w_buf.at[h, ends, x], send("xe"), recv("xe", h), facing
            ).start()
            remote(
                w_buf.at[h, other, x], w_buf.at[h, other, x], send("xy"), recv("xy", h), facing
            ).start()

        def cotangent_here(h):
            own_cotangent(h)
            across_cotangent(h)
            arrived(c_buf.at[h, ends], recv("ce", h))

        def pass_cotangent(h):
            remote(
                c_buf.at[h, ours], c_buf.at[h, ours], send("bc"), recv("bc", h), beyond
            ).start()

        def pass_over(h):
            arrived(w_buf.at[h, theirs, x], recv("bw", h))
            remote(
                w_buf.at[h, theirs, x], w_buf.at[h, theirs, x], send("xb"), recv("xb", h), facing
            ).start()

        def weights_here(h):
            arrived(w_buf.at[h, ends, xo], recv("xe", h))
            arrived(w_buf.at[h, other, xo], recv("xy", h))
            arrived(w_buf.at[h, theirs, xo], recv("xb", h))

        near, far = at(zo, y), at(zoe, y)
        near_o, far_o = at(zo, yo), at(zoe, yo)
        end_y, end_o = at(ze, y), at(ze, yo)
        late_others = (local(ze, y), local(ze, yo), other_l)

        pass_weights(0)
        early_here(near, c)
        early_copy(re_buf.at[near, c], near, c, 6, across).start()
        give_some(3, 7)
        swap_early(near, 7)
        pass_weights(1)
        early_here(other, c)
        swap_early(other, 5)
        pass_weights(2)
        keep_early.wait()
        turn(mine)
        pass_over(0)
        early_here(end_y, c)
        early_copy(re_buf.at[end_y, c], end_y, c, 2, beyond).start()
        swap_early(end_y, 3)
        for f in (other, near):
            early_here(f, co)
            turn(f)
        early_here(end_o, c)
        swap_early(end_o, 4)
        early_here(end_y, co)
        turn(end_y)
        cotangent_here(0)
        early_here(end_o, co)
        turn(end_o)

        block = 16

        def by_rows(work):
            def one(i, _):
                work(pl.ds(pl.multiple_of(i * block, block), block))
                return 0

            lax.fori_loop(0, half_rows // block, one, 0)

        def base(p):
            return 2 * hz if p == 0 else 2 * (1 - hz)

        def narrow_all():
            for p in range(2):

                def narrow(rows, p=p):
                    for side in range(2):
                        sb_buf[2 * p + side, rows] = g_buf[base(p) + side, co, rows].astype(BF)

                by_rows(narrow)
                pair = pl.ds(2 * p, 2)
                remote(
                    sb_buf.at[pair], sc_buf.at[pair], send("gc", p), recv("gc", p), partner
                ).start()

        def first_all():
            for p in range(2):
                arrived(sc_buf.at[pl.ds(2 * p, 2)], recv("gc", p))

                def first(rows, p=p):
                    sy_buf[p, rows] = (
                        g_buf[base(p) + yo, c, rows] + sc_buf[2 * p + yo, rows].astype(F32)
                    ).astype(BF)

                by_rows(first)
                remote(sy_buf.at[p], ry_buf.at[p], send("gy", p), recv("gy", p), across).start()

        def second_one(p):
            arrived(ry_buf.at[p], recv("gy", p))

            def second(rows):
                fo_buf[p, rows] = (
                    g_buf[base(p) + y, c, rows]
                    + sc_buf[2 * p + y, rows].astype(F32)
                    + ry_buf[p, rows].astype(F32)
                ).astype(BF)

            by_rows(second)
            if p == 0:
                remote(
                    fo_buf.at[0],
                    fo_buf.at[0],
                    send("ge"),
                    recv("ge"),
                    (x, at(ze, y), c),
                ).start()
            else:
                remote(fo_buf.at[1], eg_ref.at[c], send("gf"), recv("gf"), partner).start()
                pltpu.make_async_copy(fo_buf.at[1], eg_ref.at[c], recv("gl")).start()

        pres = (pre_a, pre_b)
        lag = 4

        def step(t, _):
            def taps_of(h):
                cols = columns(y, h)
                gate = [taps_ref[j : j + 1, cols] for j in range(3)]
                up = [taps_ref[j + 3 : j + 4, cols] for j in range(3)]
                return gate, up

            def project(rows, h, number):
                pres[number % 2][...] = jnp.dot(
                    rows.reshape(seq, model),
                    w_buf[h].reshape(model, 2 * LANES),
                    preferred_element_type=F32,
                ).astype(BF)

            def early(h, f, number, taps):
                gate_taps, up_taps = taps
                pre = pres[number % 2]
                gate_pre = pre[:, :LANES].astype(F32)
                up_pre = pre[:, LANES:].astype(F32)
                gate_mix = mixed(gate_pre, gate_taps)
                up_mix = mixed(up_pre, up_taps)
                cot = c_buf[h, f].astype(F32)
                square = gate_mix * gate_mix
                tanh = jnp.tanh(ROOT * gate_mix * (1.0 + CUBIC * square))
                half = 0.5 * (1.0 + tanh)
                slope = half + 0.5 * gate_mix * (1.0 - tanh * tanh) * (
                    ROOT * (1.0 + 3 * CUBIC * square)
                )
                d_gate = cot * up_mix * slope
                d_up = cot * (gate_mix * half)
                sums = []
                for grad, value in ((d_gate, gate_pre), (d_up, up_pre)):
                    for j in range(3):
                        other_value = moved_rows(value, 2 - j) if j < 2 else value
                        product = grad * other_value
                        sums.append(product.reshape(seq // 8, 8, LANES).sum(0))
                back = jnp.concatenate(
                    [
                        mixed_back(d_gate, gate_taps).astype(BF),
                        mixed_back(d_up, up_taps).astype(BF),
                    ],
                    axis=1,
                )
                return back, jnp.stack(sums)

            def late(h, fl, number, taps):
                gate_taps, up_taps = taps
                pre = pres[number % 2]
                gate_mix = mixed(pre[:, :LANES].astype(F32), gate_taps)
                up_mix = mixed(pre[:, LANES:].astype(F32), up_taps)
                tanh = jnp.tanh(ROOT * gate_mix * (1.0 + CUBIC * gate_mix * gate_mix))
                ho_buf[h, fl] = (0.5 * gate_mix * (1.0 + tanh) * up_mix).astype(BF)

            def input_grad(h, n):
                term = lax.dot_general(
                    wg_buf[h].reshape(4 * seq, 2 * LANES),
                    w_buf[h, n].reshape(seq, 2 * LANES),
                    contract_last,
                    preferred_element_type=F32,
                )
                cols = pl.ds(n * seq, seq)
                g_buf[:, :, :, cols] += term.reshape(4, 2, half_rows, seq)

            def give_out(h, kinds):
                cols = columns(y, h)
                for kind in kinds:
                    lanes = right if kind == 2 else left
                    dst = (hid_ref, gw_ref, uw_ref)[kind]

                    def src(fl):
                        if kind == 0:
                            return ho_buf.at[h, fl]
                        return wg_buf.at[h, fl, :, lanes]

                    for number, (zz, yy) in enumerate(((ze, y), (ze, yo), (zm, yo))):
                        remote(
                            src(local(zz, yy)),
                            dst.at[:, cols],
                            send("out", number * 3 + kind),
                            recv("out", y * 3 + kind),
                            (x, at(zz, yy), c),
                        ).start()
                    pltpu.make_async_copy(
                        src(mine_l), dst.at[:, cols], recv("own", kind)
                    ).start()

            def late_chunk(h, n_grads=None):
                taps = taps_of(h)
                project(rl_buf[0], h, 0)
                for fl in range(4):
                    if fl < 3:
                        project(rl_buf[fl + 1], h, fl + 1)
                    late(h, fl, fl, taps)
                    if n_grads is not None:
                        input_grad(n_grads, 2 * fl)
                        input_grad(n_grads, 2 * fl + 1)
                give_out(h, (0,))

            @pl.when(t < chunks)
            def _():
                weights_here(t)

                @pl.when(t > 0)
                def _():
                    cotangent_here(t)

                @pl.when(t + 1 < chunks)
                def _():
                    pass_over(t + 1)

                taps = taps_of(t)
                first = 4 * hz
                project(re_buf[first], t, 0)
                for fl in range(4):
                    if fl < 3:
                        project(re_buf[first + fl + 1], t, fl + 1)
                    back, sums = early(t, first + fl, fl, taps)
                    wg_buf[t, fl] = back
                    if fl == 0:
                        ts_buf[t] = sums
                    else:
                        ts_buf[t] += sums

            @pl.when(t == 0)
            def _():
                early_here(far, c)
                early_copy(re_buf.at[far, c], far, c, 8, across).start()
                give_across(7)
                late_copy(late_ref.at[c], mine_l, c, 12, across).start()
                give_some(8, chunks)
                swap_early(far, 9)

            @pl.when(t + 3 < chunks)
            def _():
                pass_weights(t + 3)

            @pl.when(t < chunks)
            def _():
                pass_cotangent(t)

            @pl.when(t == 2)
            def _():
                early_here(near_o, c)
                swap_early(near_o, 10)
                early_here(far, co)
                turn(far)
                early_here(near_o, co)
                turn(near_o)

            @pl.when(t == 3)
            def _():
                early_here(far_o, c)
                swap_early(far_o, 11)
                early_here(far_o, co)
                turn(far_o)

            @pl.when(t == 6)
            def _():
                for fl, number in zip(late_others, (13, 14, 15)):
                    late_here(fl, c)
                    swap_late(fl, number)
                keep_late.wait()
                for fl in late_others:
                    late_here(fl, co)

            @pl.when(t < 6)
            def _():
                for n in range(8):
                    input_grad(t, n)

            odd = t % 2
            late_first = 3 * (t - 6 - odd) // 2 + 2 * odd

            @pl.when((t >= 6) & (t < chunks))
            def _():
                late_chunk(late_first, t)

            @pl.when((t >= chunks) & (late_first < chunks))
            def _():
                late_chunk(late_first)

            @pl.when((t >= 6) & (odd == 0) & (late_first + 1 < chunks))
            def _():
                late_chunk(late_first + 1)

            @pl.when(t == chunks - 1)
            def _():
                narrow_all()

            @pl.when(t == chunks)
            def _():
                first_all()

            @pl.when(t == chunks + 3)
            def _():
                second_one(0)

            @pl.when(t >= lag)
            def _():
                h = t - lag
                arrived(c_buf.at[h, theirs], recv("bc", h))
                for fl in range(4):
                    dp_buf[4 * hz + fl] = wg_buf[h, fl]
                taps = taps_of(h)
                first = 4 * (1 - hz)
                total = None
                project(re_buf[first], h, 0)
                for fl in range(4):
                    if fl < 3:
                        project(re_buf[first + fl + 1], h, fl + 1)
                    back, sums = early(h, first + fl, fl, taps)
                    dp_buf[first + fl] = back
                    total = sums if total is None else total + sums
                total = ts_buf[h] + total
                here = pl.ds(pl.multiple_of(h * LANES, LANES), LANES)
                tt_buf[pl.ds(0, 6), here] = jnp.sum(total, axis=1)
                for fl in range(4):
                    product = jnp.dot(
                        rt_buf[fl],
                        dp_buf[...].reshape(8 * seq, 2 * LANES),
                        preferred_element_type=F32,
                    )
                    wg_buf[h, fl] = (product * scale).astype(BF)
                give_out(h, (1, 2))

            return 0

        lax.fori_loop(0, chunks + lag, step, 0)
        for number, (zz, yy) in enumerate(((ze, y), (ze, yo), (zm, yo))):
            remote(
                tt_buf,
                tap_ref.at[y],
                send("tap", number),
                recv("tap", y),
                (x, at(zz, yy), c),
            ).start()
        pltpu.make_async_copy(tt_buf, tap_ref.at[y], recv("owntap")).start()
        second_one(1)

        for number in range(16):
            sent(early_ref.at[c], send("rows", number))
        across_sent()
        sent(w_buf.at[:, ours, x], send("bw"))
        sent(w_buf.at[:, ends, x], send("xe"))
        sent(w_buf.at[:, other, x], send("xy"))
        sent(w_buf.at[:, theirs, x], send("xb"))
        sent(c_buf.at[:, ours], send("bc"))
        for number, (zz, yy) in enumerate(((ze, y), (ze, yo), (zm, yo))):
            fl = local(zz, yy)
            sent(ho_buf.at[:, fl], send("out", number * 3))
            sent(wg_buf.at[:, fl, :, left], send("out", number * 3 + 1))
            sent(wg_buf.at[:, fl, :, right], send("out", number * 3 + 2))
            sent(tt_buf, send("tap", number))
        for p in range(2):
            sent(sb_buf.at[pl.ds(2 * p, 2)], send("gc", p))
            sent(sy_buf.at[p], send("gy", p))
        sent(fo_buf.at[0], send("ge"))
        sent(fo_buf.at[1], send("gf"))
        copied(eg_ref.at[c], recv("gl"))
        arrived(eg_ref.at[co], recv("gf"))
        for kind, ref in enumerate((hid_ref, gw_ref, uw_ref)):
            copied(ref.at[:, whole(y)], recv("own", kind))
            arrived(ref.at[:, whole(yo)], recv("out", yo * 3 + kind))
        copied(tap_ref.at[y], recv("owntap"))
        arrived(tap_ref.at[yo], recv("tap", yo))


def by_halves(
    late_rows,
    early_rows,
    hidden_cot,
    gate_weight,
    up_weight,
    gate_taps,
    up_taps,
    gate_grad_sum,
    up_grad_sum,
    gate_taps_sum,
    up_taps_sum,
):
    fs_size = lax.axis_size("fs")
    rows, model = late_rows.shape
    width = gate_weight.shape[1]
    span = width // 2
    chunks = span // LANES
    half_rows = rows // 2
    scale = (rows * fs_size) ** (-0.5)
    plan = Plan(chunks)
    taps = jnp.concatenate([gate_taps, up_taps], axis=0).astype(F32)
    anywhere = pl.BlockSpec(memory_space=pl.ANY)
    vmem = pltpu.VMEM
    hidden, grad, gate_sum, up_sum, tap_sum = pl.pallas_call(
        functools.partial(layer_kernel, plan, scale),
        out_shape=(
            jax.ShapeDtypeStruct((rows, width), BF),
            jax.ShapeDtypeStruct((2, half_rows, model), BF),
            jax.ShapeDtypeStruct((rows, width), BF),
            jax.ShapeDtypeStruct((rows, width), BF),
            jax.ShapeDtypeStruct((2, 8, span), F32),
        ),
        in_specs=[anywhere] * 5 + [pl.BlockSpec(memory_space=vmem)],
        out_specs=(anywhere,) * 5,
        scratch_shapes=[
            vmem((chunks, fs_size, 2, half_rows, 2 * LANES), BF),
            vmem((chunks, fs_size, rows, LANES), BF),
            vmem((fs_size, 2, half_rows, model), BF),
            vmem((fs_size // 2, 2, half_rows, model), BF),
            vmem((fs_size // 2, rows, fs_size * rows), BF),
            vmem((fs_size, rows, 2 * LANES), BF),
            vmem((fs_size // 2, 2, half_rows, model), F32),
            vmem((chunks, fs_size // 2, rows, LANES), BF),
            vmem((chunks, fs_size // 2, rows, 2 * LANES), BF),
            vmem((chunks, 6, 8, LANES), F32),
            vmem((8, span), F32),
            vmem((rows, 2 * LANES), BF),
            vmem((rows, 2 * LANES), BF),
            vmem((4, half_rows, model), BF),
            vmem((4, half_rows, model), BF),
            vmem((2, half_rows, model), BF),
            vmem((2, half_rows, model), BF),
            vmem((2, half_rows, model), BF),
            pltpu.SemaphoreType.DMA((plan.send_count,)),
            pltpu.SemaphoreType.DMA((plan.recv_count,)),
        ],
        compiler_params=pltpu.CompilerParams(
            has_side_effects=True, vmem_limit_bytes=67043328
        ),
    )(
        late_rows.reshape(2, half_rows, model),
        early_rows.reshape(2, half_rows, model),
        hidden_cot,
        gate_weight.reshape(2, half_rows, width),
        up_weight.reshape(2, half_rows, width),
        taps,
    )
    tap_sum = scale * jnp.concatenate([tap_sum[0, :6], tap_sum[1, :6]], axis=1)
    return (
        hidden,
        grad.reshape(rows, model),
        gate_grad_sum + gate_sum.astype(F32),
        up_grad_sum + up_sum.astype(F32),
        gate_taps_sum + tap_sum[:3],
        up_taps_sum + tap_sum[3:],
    )


def solution(mesh):
    in_specs = (
        P(("rep", "fs"), None),
        P(("rep", "fs"), None),
        P(("rep", "fs"), "tp"),
        P("fs", "tp"),
        P("fs", "tp"),
        P(None, "tp"),
        P(None, "tp"),
        P(("rep", "fs"), "tp"),
        P(("rep", "fs"), "tp"),
        P("rep", "tp"),
        P("rep", "tp"),
    )
    out_specs = (
        P(("rep", "fs"), "tp"),
        P(("rep", "fs"), None),
        P(("rep", "fs"), "tp"),
        P(("rep", "fs"), "tp"),
        P("rep", "tp"),
        P("rep", "tp"),
    )
    sizes = dict(mesh.shape)

    def run(*args):
        rows = args[0].shape[0] // (sizes["rep"] * sizes["fs"])
        model = args[0].shape[1]
        width = args[3].shape[1] // sizes["tp"]
        small = rows <= 256 and model <= 2048 and width <= 2816
        even = rows % 256 == 0 and width % (2 * LANES) == 0 and model == 8 * rows
        small = small and 9 <= width // (2 * LANES) <= 11
        fits = (sizes["rep"], sizes["fs"], sizes["tp"]) == (2, 8, 2) and small and even
        return jax.shard_map(
            by_halves if fits else per_device,
            mesh=mesh,
            in_specs=in_specs,
            out_specs=out_specs,
            check_vma=False,
        )(*args)

    return run
```

```python
import functools
import math

import jax
import jax.numpy as jnp
from jax import lax
from jax.experimental import pallas as pl
from jax.experimental.pallas import tpu as pltpu
from jax.sharding import PartitionSpec as P

contract_last = (((1,), (1,)), ((), ()))
contract_first = (((0,), (0,)), ((), ()))


BF, F32 = jnp.bfloat16, jnp.float32
MESH = pl.DeviceIdType.MESH
LANES = 128
ROOT = math.sqrt(2 / math.pi)
CUBIC = 0.044715


def causal_mix(values, filter_taps):
    length = values.shape[-2]
    widths = [(0, 0)] * values.ndim
    widths[-2] = (2, 0)
    padded = jnp.pad(values, widths)
    return (
        filter_taps[0] * padded[..., 0:length, :]
        + filter_taps[1] * padded[..., 1 : length + 1, :]
        + filter_taps[2] * padded[..., 2 : length + 2, :]
    )


def mix_back(grads, filter_taps):
    length = grads.shape[-2]
    widths = [(0, 0)] * grads.ndim
    widths[-2] = (0, 2)
    padded = jnp.pad(grads, widths)
    return (
        filter_taps[2] * padded[..., 0:length, :]
        + filter_taps[1] * padded[..., 1 : length + 1, :]
        + filter_taps[0] * padded[..., 2 : length + 2, :]
    )


def tap_products(grads, values):
    length = values.shape[-2]
    widths = [(0, 0)] * values.ndim
    widths[-2] = (2, 0)
    padded = jnp.pad(values, widths)
    axes = tuple(range(values.ndim - 1))
    return jnp.stack(
        [
            jnp.sum(grads * padded[..., offset : offset + length, :], axis=axes)
            for offset in range(3)
        ]
    )


def stored(product):
    return lax.optimization_barrier(product.astype(jnp.bfloat16)).astype(jnp.float32)


def per_device(
    late_rows,
    early_rows,
    hidden_cot,
    gate_weight,
    up_weight,
    gate_taps,
    up_taps,
    gate_grad_sum,
    up_grad_sum,
    gate_taps_sum,
    up_taps_sum,
):
    row_count = late_rows.shape[0]
    width_local = gate_weight.shape[1]
    rows_scale = (row_count * lax.axis_size("fs")) ** (-0.5)
    gate_filter = gate_taps.astype(jnp.float32)
    up_filter = up_taps.astype(jnp.float32)
    joined_weight = jnp.concatenate([gate_weight, up_weight], axis=1)
    both_rows = jnp.concatenate([late_rows, early_rows], axis=0)
    whole_joined = lax.all_gather(joined_weight, "fs", axis=0, tiled=True)
    projected = jnp.dot(both_rows, whole_joined, preferred_element_type=jnp.float32)
    projected = stored(projected)
    late_gate = projected[:row_count, :width_local]
    late_up = projected[:row_count, width_local:]
    early_gate = projected[row_count:, :width_local]
    early_up = projected[row_count:, width_local:]
    late_hidden = (
        jax.nn.gelu(causal_mix(late_gate, gate_filter), approximate=True)
        * causal_mix(late_up, up_filter)
    ).astype(jnp.bfloat16)
    gate_mix = causal_mix(early_gate, gate_filter)
    up_mix = causal_mix(early_up, up_filter)
    cotangent = hidden_cot.astype(jnp.float32)
    activated, gelu_back = jax.vjp(
        lambda mixed_value: jax.nn.gelu(mixed_value, approximate=True), gate_mix
    )
    d_gate_mix = gelu_back(cotangent * up_mix)[0]
    d_up_mix = cotangent * activated
    d_gate_pre = mix_back(d_gate_mix, gate_filter).astype(jnp.bfloat16)
    d_up_pre = mix_back(d_up_mix, up_filter).astype(jnp.bfloat16)
    both_grads = jnp.concatenate([d_gate_pre, d_up_pre], axis=1)
    early_grad = lax.psum(
        lax.dot_general(
            both_grads, whole_joined, contract_last, preferred_element_type=jnp.float32
        ).astype(jnp.bfloat16),
        "tp",
    )
    summed = lax.psum_scatter(
        (
            lax.dot_general(
                early_rows, both_grads, contract_first, preferred_element_type=jnp.float32
            )
            * rows_scale
        ).astype(jnp.bfloat16),
        "fs",
        scatter_dimension=0,
        tiled=True,
    ).astype(jnp.float32)
    gate_tap_sums, up_tap_sums = lax.psum(
        (
            rows_scale * tap_products(d_gate_mix, early_gate),
            rows_scale * tap_products(d_up_mix, early_up),
        ),
        "fs",
    )
    return (
        late_hidden,
        early_grad,
        gate_grad_sum + summed[:, :width_local],
        up_grad_sum + summed[:, width_local:],
        gate_taps_sum + gate_tap_sums,
        up_taps_sum + up_tap_sums,
    )


def moved_rows(values, count):
    rows = lax.broadcasted_iota(jnp.int32, values.shape, 0)
    length = values.shape[0]
    if count > 0:
        return jnp.where(rows >= count, pltpu.roll(values, count, 0), 0.0)
    return jnp.where(rows < length + count, pltpu.roll(values, length + count, 0), 0.0)


def mixed(values, taps):
    return (
        taps[0] * moved_rows(values, 2) + taps[1] * moved_rows(values, 1) + taps[2] * values
    )


def mixed_back(values, taps):
    return (
        taps[2] * values + taps[1] * moved_rows(values, -1) + taps[0] * moved_rows(values, -2)
    )


CHUNK_RECV = ("we", "ce", "wyg", "wyu", "cy", "lg", "lu", "lc", "xe", "xy", "bw", "bc", "xb")
CHUNK_SEND = ("wyg", "wyu", "cy", "we", "ce", "xe", "xy", "bw", "bc", "xb")


class Plan:
    def __init__(self, chunks):
        self.chunks = chunks
        self.recv, self.send = {}, {}
        self.recv_count = self.send_count = 0
        self.add_recv("re", 16)
        self.add_recv("rl", 8)
        for name in CHUNK_RECV:
            self.add_recv(name, chunks)
        self.add_recv("out", 6)
        self.add_recv("own", 3)
        self.add_recv("tap", 2)
        self.add_recv("owntap", 1)
        self.add_recv("gc", 2)
        self.add_recv("gy", 2)
        self.add_recv("ge", 1)
        self.add_recv("gf", 1)
        self.add_recv("gl", 1)
        for name in CHUNK_SEND:
            self.add_send(name, 1)
        self.add_send("rows", 24)
        self.add_send("out", 9)
        self.add_send("tap", 3)
        self.add_send("gc", 2)
        self.add_send("gy", 2)
        self.add_send("ge", 1)
        self.add_send("gf", 1)

    def add_recv(self, name, count):
        self.recv[name] = self.recv_count
        self.recv_count += count

    def add_send(self, name, count):
        self.send[name] = self.send_count
        self.send_count += count


def layer_kernel(
    plan,
    scale,
    late_ref,
    early_ref,
    cot_ref,
    gate_ref,
    up_ref,
    taps_ref,
    hid_ref,
    eg_ref,
    gw_ref,
    uw_ref,
    tap_ref,
    w_buf,
    c_buf,
    re_buf,
    rl_buf,
    rt_buf,
    dp_buf,
    g_buf,
    ho_buf,
    wg_buf,
    ts_buf,
    tt_buf,
    pre_a,
    pre_b,
    sb_buf,
    sc_buf,
    sy_buf,
    ry_buf,
    fo_buf,
    send_sems,
    recv_sems,
):
    chunks = plan.chunks
    span = chunks * LANES
    model = re_buf.shape[3]
    half_rows = re_buf.shape[2]
    seq = 2 * half_rows
    x = lax.axis_index("rep")
    fs = lax.axis_index("fs")
    c = lax.axis_index("tp")
    z = fs // 2
    y = fs % 2
    hz = z // 2
    xo, yo, co = 1 - x, 1 - y, 1 - c
    zm, ze, zo = 1 + hz, 3 * hz, 2 - hz
    zoe = 3 - ze
    is_mid = z == zm
    is_end = z == ze

    def at(zz, yy):
        return zz * 2 + yy

    def local(zz, yy):
        return (zz - 2 * hz) * 2 + yy

    def recv(name, index=0):
        return recv_sems.at[plan.recv[name] + index]

    def send(name, index=0):
        return send_sems.at[plan.send[name] + index]

    def remote(src, dst, send_sem, recv_sem, target):
        return pltpu.make_async_remote_copy(
            src_ref=src,
            dst_ref=dst,
            send_sem=send_sem,
            recv_sem=recv_sem,
            device_id=target,
            device_id_type=MESH,
        )

    partner = (x, fs, co)
    across = (x, at(z, yo), c)
    facing = (xo, fs, c)
    home = (x, at(zm, y), c)
    beyond = (x, at(zo, y), c)

    def arrived(ref, sem):
        remote(ref, ref, send("rows"), sem, partner).wait_recv()

    def sent(ref, sem):
        remote(ref, ref, sem, recv("re"), partner).wait_send()

    def copied(ref, sem):
        pltpu.make_async_copy(ref, ref, sem).wait()

    def columns(side, h):
        return pl.ds(pl.multiple_of(side * span + h * LANES, LANES), LANES)

    whole = lambda side: pl.ds(pl.multiple_of(side * span, LANES), span)
    left, right = pl.ds(0, LANES), pl.ds(LANES, LANES)
    ends = pl.ds(2 * ze, 2)
    ours = pl.ds(4 * hz, 4)
    theirs = pl.ds(4 * (1 - hz), 4)

    def gather_own(h, rows):
        pltpu.make_async_copy(
            gate_ref.at[rows, :, columns(y, h)], w_buf.at[h, fs, rows, :, left], recv("lg", h)
        ).start()
        pltpu.make_async_copy(
            up_ref.at[rows, :, columns(y, h)], w_buf.at[h, fs, rows, :, right], recv("lu", h)
        ).start()
        pltpu.make_async_copy(
            cot_ref.at[:, columns(y, h)], c_buf.at[h, fs], recv("lc", h)
        ).start()

    def own_weights(h, rows):
        copied(w_buf.at[h, fs, rows, :, left], recv("lg", h))
        copied(w_buf.at[h, fs, rows, :, right], recv("lu", h))

    def own_cotangent(h):
        copied(c_buf.at[h, fs], recv("lc", h))

    def give_across(h):
        remote(
            gate_ref.at[x, :, columns(yo, h)],
            w_buf.at[h, fs, x, :, left],
            send("wyg"),
            recv("wyg", h),
            across,
        ).start()
        remote(
            up_ref.at[x, :, columns(yo, h)],
            w_buf.at[h, fs, x, :, right],
            send("wyu"),
            recv("wyu", h),
            across,
        ).start()
        remote(
            cot_ref.at[:, columns(yo, h)],
            c_buf.at[h, fs],
            send("cy"),
            recv("cy", h),
            across,
        ).start()

    def across_weights(h):
        other = at(z, yo)
        arrived(w_buf.at[h, other, x, :, left], recv("wyg", h))
        arrived(w_buf.at[h, other, x, :, right], recv("wyu", h))

    def across_cotangent(h):
        arrived(c_buf.at[h, at(z, yo)], recv("cy", h))

    def give_some(first, last):
        def one(h, _):
            give_across(h)
            return 0

        lax.fori_loop(first, last, one, 0)

    def across_sent():
        sent(gate_ref.at[x, :, whole(yo)], send("wyg"))
        sent(up_ref.at[x, :, whole(yo)], send("wyu"))
        sent(cot_ref.at[:, whole(yo)], send("cy"))

    def early_copy(src, f, half, number, target):
        return remote(
            src, re_buf.at[f, half], send("rows", number), recv("re", f * 2 + half), target
        )

    def late_copy(src, fl, half, number, target):
        return remote(
            src, rl_buf.at[fl, half], send("rows", number), recv("rl", fl * 2 + half), target
        )

    def early_here(f, half):
        arrived(re_buf.at[f, half], recv("re", f * 2 + half))

    def late_here(fl, half):
        arrived(rl_buf.at[fl, half], recv("rl", fl * 2 + half))

    @pl.when(is_end)
    def _():
        mine, other = at(ze, y), at(ze, yo)
        mine_l, other_l = local(ze, y), local(ze, yo)

        def own(h, _):
            gather_own(h, x)
            return 0

        def hand_weights(h):
            own_weights(h, x)
            across_weights(h)
            remote(
                w_buf.at[h, ends, x], w_buf.at[h, ends, x], send("we"), recv("we", h), home
            ).start()

        def hand_cotangent(h):
            own_cotangent(h)
            across_cotangent(h)
            remote(
                c_buf.at[h, ends], c_buf.at[h, ends], send("ce"), recv("ce", h), home
            ).start()

        give_across(0)
        gather_own(0, x)
        give_across(1)
        early_copy(early_ref.at[c], mine, c, 1, across).start()
        gather_own(1, x)
        hand_weights(0)
        early_copy(early_ref.at[c], mine, c, 0, home).start()
        give_some(2, 6)
        late_copy(late_ref.at[c], mine_l, c, 2, across).start()
        give_some(6, chunks)
        lax.fori_loop(2, chunks, own, 0)

        hand_weights(1)
        hand_cotangent(0)
        early_here(other, c)
        early_copy(re_buf.at[other, c], other, c, 3, home).start()
        for h in range(2, 4):
            hand_weights(h)
            hand_cotangent(h - 1)
        hand_weights(4)
        hand_weights(5)
        hand_cotangent(3)
        late_copy(late_ref.at[c], mine_l, c, 4, home).start()
        hand_weights(6)
        hand_cotangent(4)
        late_here(other_l, c)
        late_copy(rl_buf.at[other_l, c], other_l, c, 5, home).start()
        hand_weights(7)
        hand_cotangent(5)
        hand_weights(8)

        def each(h, _):
            hand_weights(h)
            hand_cotangent(h - 3)
            return 0

        lax.fori_loop(9, chunks, each, 0)
        for h in range(chunks - 3, chunks):
            hand_cotangent(h)

        sent(early_ref.at[c], send("rows", 0))
        sent(early_ref.at[c], send("rows", 1))
        sent(late_ref.at[c], send("rows", 2))
        sent(early_ref.at[c], send("rows", 3))
        sent(late_ref.at[c], send("rows", 4))
        sent(late_ref.at[c], send("rows", 5))
        across_sent()
        sent(w_buf.at[:, ends, x], send("we"))
        sent(c_buf.at[:, ends], send("ce"))

        arrived(fo_buf.at[0], recv("ge"))
        remote(fo_buf.at[0], eg_ref.at[c], send("gf"), recv("gf"), partner).start()
        keep = pltpu.make_async_copy(fo_buf.at[0], eg_ref.at[c], recv("gl"))
        keep.start()
        keep.wait()
        sent(fo_buf.at[0], send("gf"))
        arrived(eg_ref.at[co], recv("gf"))

        for side in range(2):
            arrived(hid_ref.at[:, pl.ds(side * span, span)], recv("out", side * 3))
            arrived(gw_ref.at[:, pl.ds(side * span, span)], recv("out", side * 3 + 1))
            arrived(uw_ref.at[:, pl.ds(side * span, span)], recv("out", side * 3 + 2))
            arrived(tap_ref.at[:, pl.ds(side * span, span)], recv("tap", side))

    @pl.when(is_mid)
    def _():
        mine, other = at(zm, y), at(zm, yo)
        mine_l, other_l = local(zm, y), local(zm, yo)
        both = pl.ds(0, 2)

        give_across(0)
        early_copy(early_ref.at[c], mine, c, 0, beyond).start()
        early_copy(early_ref.at[c], mine, c, 1, across).start()
        give_across(1)
        gather_own(0, both)
        keep_early = pltpu.make_async_copy(early_ref, re_buf.at[mine], recv("re", mine * 2))
        keep_late = pltpu.make_async_copy(late_ref, rl_buf.at[mine_l], recv("rl", mine_l * 2))
        keep_early.start()

        def own(h, _):
            gather_own(h, both)
            return 0

        lax.fori_loop(1, chunks, own, 0)
        keep_late.start()

        def clear(fl, _):
            g_buf[fl] = jnp.zeros_like(g_buf[0])
            return 0

        lax.fori_loop(0, 4, clear, 0)

        def turn(f):
            def one(fl, _):
                cols = pl.ds(pl.multiple_of((4 * hz + fl) * seq, LANES), seq)
                block = re_buf[f, :, :, cols].reshape(seq, seq)
                rt_buf[fl, :, pl.ds(pl.multiple_of(f * seq, LANES), seq)] = block.T
                return 0

            lax.fori_loop(0, 4, one, 0)

        def swap_early(f, number):
            early_copy(re_buf.at[f, c], f, c, number, partner).start()

        def swap_late(fl, number):
            late_copy(rl_buf.at[fl, c], fl, c, number, partner).start()

        def pass_weights(h):
            own_weights(h, both)
            across_weights(h)
            arrived(w_buf.at[h, ends, x], recv("we", h))
            remote(
                w_buf.at[h, ours, x], w_buf.at[h, ours, x], send("bw"), recv("bw", h), beyond
            ).start()
            remote(
                w_buf.at[h, ends, x], w_buf.at[h, ends, x], send("xe"), recv("xe", h), facing
            ).start()
            remote(
                w_buf.at[h, other, x], w_buf.at[h, other, x], send("xy"), recv("xy", h), facing
            ).start()

        def cotangent_here(h):
            own_cotangent(h)
            across_cotangent(h)
            arrived(c_buf.at[h, ends], recv("ce", h))

        def pass_cotangent(h):
            remote(
                c_buf.at[h, ours], c_buf.at[h, ours], send("bc"), recv("bc", h), beyond
            ).start()

        def pass_over(h):
            arrived(w_buf.at[h, theirs, x], recv("bw", h))
            remote(
                w_buf.at[h, theirs, x], w_buf.at[h, theirs, x], send("xb"), recv("xb", h), facing
            ).start()

        def weights_here(h):
            arrived(w_buf.at[h, ends, xo], recv("xe", h))
            arrived(w_buf.at[h, other, xo], recv("xy", h))
            arrived(w_buf.at[h, theirs, xo], recv("xb", h))

        near, far = at(zo, y), at(zoe, y)
        near_o, far_o = at(zo, yo), at(zoe, yo)
        end_y, end_o = at(ze, y), at(ze, yo)
        late_others = (local(ze, y), local(ze, yo), other_l)

        pass_weights(0)
        early_here(near, c)
        early_copy(re_buf.at[near, c], near, c, 6, across).start()
        give_across(2)
        swap_early(near, 7)
        early_here(other, c)
        swap_early(other, 5)
        keep_early.wait()
        turn(mine)
        early_here(end_y, c)
        early_copy(re_buf.at[end_y, c], end_y, c, 2, beyond).start()
        swap_early(end_y, 3)
        pass_weights(1)
        cotangent_here(0)
        pass_cotangent(0)
        pass_over(0)
        for f in (other, near):
            early_here(f, co)
            turn(f)
        early_here(far, c)
        early_copy(re_buf.at[far, c], far, c, 8, across).start()
        give_some(3, 5)
        late_copy(late_ref.at[c], mine_l, c, 12, across).start()
        give_some(5, chunks)
        swap_early(far, 9)
        early_here(end_y, co)
        turn(end_y)
        early_here(end_o, c)
        swap_early(end_o, 4)
        pass_weights(2)
        early_here(end_o, co)
        turn(end_o)

        block = 16

        def by_rows(work):
            def one(i, _):
                work(pl.ds(pl.multiple_of(i * block, block), block))
                return 0

            lax.fori_loop(0, half_rows // block, one, 0)

        def base(p):
            return 2 * hz if p == 0 else 2 * (1 - hz)

        def narrow_all():
            for p in range(2):

                def narrow(rows, p=p):
                    for side in range(2):
                        sb_buf[2 * p + side, rows] = g_buf[base(p) + side, co, rows].astype(BF)

                by_rows(narrow)
                pair = pl.ds(2 * p, 2)
                remote(
                    sb_buf.at[pair], sc_buf.at[pair], send("gc", p), recv("gc", p), partner
                ).start()

        def first_all():
            for p in range(2):
                arrived(sc_buf.at[pl.ds(2 * p, 2)], recv("gc", p))

                def first(rows, p=p):
                    sy_buf[p, rows] = (
                        g_buf[base(p) + yo, c, rows] + sc_buf[2 * p + yo, rows].astype(F32)
                    ).astype(BF)

                by_rows(first)
                remote(sy_buf.at[p], ry_buf.at[p], send("gy", p), recv("gy", p), across).start()

        def second_one(p):
            arrived(ry_buf.at[p], recv("gy", p))

            def second(rows):
                fo_buf[p, rows] = (
                    g_buf[base(p) + y, c, rows]
                    + sc_buf[2 * p + y, rows].astype(F32)
                    + ry_buf[p, rows].astype(F32)
                ).astype(BF)

            by_rows(second)
            if p == 0:
                remote(
                    fo_buf.at[0],
                    fo_buf.at[0],
                    send("ge"),
                    recv("ge"),
                    (x, at(ze, y), c),
                ).start()
            else:
                remote(fo_buf.at[1], eg_ref.at[c], send("gf"), recv("gf"), partner).start()
                pltpu.make_async_copy(fo_buf.at[1], eg_ref.at[c], recv("gl")).start()

        pres = (pre_a, pre_b)
        lag = 3

        def step(t, _):
            def taps_of(h):
                cols = columns(y, h)
                gate = [taps_ref[j : j + 1, cols] for j in range(3)]
                up = [taps_ref[j + 3 : j + 4, cols] for j in range(3)]
                return gate, up

            def project(rows, h, number):
                pres[number % 2][...] = jnp.dot(
                    rows.reshape(seq, model),
                    w_buf[h].reshape(model, 2 * LANES),
                    preferred_element_type=F32,
                ).astype(BF)

            def early(h, f, number, taps):
                gate_taps, up_taps = taps
                pre = pres[number % 2]
                gate_pre = pre[:, :LANES].astype(F32)
                up_pre = pre[:, LANES:].astype(F32)
                gate_mix = mixed(gate_pre, gate_taps)
                up_mix = mixed(up_pre, up_taps)
                cot = c_buf[h, f].astype(F32)
                square = gate_mix * gate_mix
                tanh = jnp.tanh(ROOT * gate_mix * (1.0 + CUBIC * square))
                half = 0.5 * (1.0 + tanh)
                slope = half + 0.5 * gate_mix * (1.0 - tanh * tanh) * (
                    ROOT * (1.0 + 3 * CUBIC * square)
                )
                d_gate = cot * up_mix * slope
                d_up = cot * (gate_mix * half)
                sums = []
                for grad, value in ((d_gate, gate_pre), (d_up, up_pre)):
                    for j in range(3):
                        other_value = moved_rows(value, 2 - j) if j < 2 else value
                        product = grad * other_value
                        sums.append(product.reshape(seq // 8, 8, LANES).sum(0))
                back = jnp.concatenate(
                    [
                        mixed_back(d_gate, gate_taps).astype(BF),
                        mixed_back(d_up, up_taps).astype(BF),
                    ],
                    axis=1,
                )
                return back, jnp.stack(sums)

            def late(h, fl, number, taps):
                gate_taps, up_taps = taps
                pre = pres[number % 2]
                gate_mix = mixed(pre[:, :LANES].astype(F32), gate_taps)
                up_mix = mixed(pre[:, LANES:].astype(F32), up_taps)
                tanh = jnp.tanh(ROOT * gate_mix * (1.0 + CUBIC * gate_mix * gate_mix))
                ho_buf[h, fl] = (0.5 * gate_mix * (1.0 + tanh) * up_mix).astype(BF)

            def input_grad(h, n):
                term = lax.dot_general(
                    wg_buf[h].reshape(4 * seq, 2 * LANES),
                    w_buf[h, n].reshape(seq, 2 * LANES),
                    contract_last,
                    preferred_element_type=F32,
                )
                cols = pl.ds(n * seq, seq)
                g_buf[:, :, :, cols] += term.reshape(4, 2, half_rows, seq)

            def give_out(h, kinds):
                cols = columns(y, h)
                for kind in kinds:
                    lanes = right if kind == 2 else left
                    dst = (hid_ref, gw_ref, uw_ref)[kind]

                    def src(fl):
                        if kind == 0:
                            return ho_buf.at[h, fl]
                        return wg_buf.at[h, fl, :, lanes]

                    for number, (zz, yy) in enumerate(((ze, y), (ze, yo), (zm, yo))):
                        remote(
                            src(local(zz, yy)),
                            dst.at[:, cols],
                            send("out", number * 3 + kind),
                            recv("out", y * 3 + kind),
                            (x, at(zz, yy), c),
                        ).start()
                    pltpu.make_async_copy(
                        src(mine_l), dst.at[:, cols], recv("own", kind)
                    ).start()

            def late_chunk(h, n_grads=None):
                taps = taps_of(h)
                project(rl_buf[0], h, 0)
                for fl in range(4):
                    if fl < 3:
                        project(rl_buf[fl + 1], h, fl + 1)
                    late(h, fl, fl, taps)
                    if n_grads is not None:
                        input_grad(n_grads, 2 * fl)
                        input_grad(n_grads, 2 * fl + 1)
                give_out(h, (0,))

            @pl.when(t < chunks)
            def _():
                weights_here(t)

                @pl.when(t + 1 < chunks)
                def _():
                    pass_over(t + 1)

                taps = taps_of(t)
                first = 4 * hz
                project(re_buf[first], t, 0)
                for fl in range(4):
                    if fl < 3:
                        project(re_buf[first + fl + 1], t, fl + 1)
                    back, sums = early(t, first + fl, fl, taps)
                    wg_buf[t, fl] = back
                    if fl == 0:
                        ts_buf[t] = sums
                    else:
                        ts_buf[t] += sums

            @pl.when(t == 0)
            def _():
                early_here(near_o, c)
                swap_early(near_o, 10)
                early_here(far, co)
                turn(far)

            @pl.when(t == 1)
            def _():
                early_here(far_o, c)
                swap_early(far_o, 11)
                early_here(near_o, co)
                turn(near_o)
                early_here(far_o, co)
                turn(far_o)

            @pl.when(t == 4)
            def _():
                for fl, number in zip(late_others, (13, 14, 15)):
                    late_here(fl, c)
                    swap_late(fl, number)
                keep_late.wait()
                for fl in late_others:
                    late_here(fl, co)

            late_first = jnp.where(t < 8, 2 * (t - 4), t)

            @pl.when(t < 4)
            def _():
                for n in range(8):
                    input_grad(t, n)

            @pl.when((t >= 4) & (t < chunks))
            def _():
                late_chunk(late_first, t)

            @pl.when((t >= 4) & (t < 8))
            def _():
                late_chunk(late_first + 1)

            @pl.when(t == chunks - 1)
            def _():
                narrow_all()

            @pl.when(t == chunks)
            def _():
                first_all()

            @pl.when(t == chunks + 1)
            def _():
                second_one(0)

            @pl.when(t == 0)
            def _():
                cotangent_here(1)
                pass_cotangent(1)

            @pl.when(t == 1)
            def _():
                pass_weights(3)

            @pl.when((t >= 1) & (t != 4))
            def _():
                h = jnp.where(t < 4, t - 1, t - lag + 1)
                arrived(c_buf.at[h, theirs], recv("bc", h))
                for fl in range(4):
                    dp_buf[4 * hz + fl] = wg_buf[h, fl]
                taps = taps_of(h)
                first = 4 * (1 - hz)
                total = None
                project(re_buf[first], h, 0)
                for fl in range(4):
                    if fl < 3:
                        project(re_buf[first + fl + 1], h, fl + 1)
                    back, sums = early(h, first + fl, fl, taps)
                    dp_buf[first + fl] = back
                    total = sums if total is None else total + sums
                total = ts_buf[h] + total
                here = pl.ds(pl.multiple_of(h * LANES, LANES), LANES)
                tt_buf[pl.ds(0, 6), here] = jnp.sum(total, axis=1)
                for fl in range(4):
                    product = jnp.dot(
                        rt_buf[fl],
                        dp_buf[...].reshape(8 * seq, 2 * LANES),
                        preferred_element_type=F32,
                    )
                    wg_buf[h, fl] = (product * scale).astype(BF)
                give_out(h, (1, 2))

            @pl.when((t >= 1) & (t + 3 < chunks))
            def _():
                pass_weights(t + 3)

            @pl.when((t >= 1) & (t + 1 < chunks))
            def _():
                cotangent_here(t + 1)
                pass_cotangent(t + 1)

            return 0

        lax.fori_loop(0, chunks + lag - 1, step, 0)
        for number, (zz, yy) in enumerate(((ze, y), (ze, yo), (zm, yo))):
            remote(
                tt_buf,
                tap_ref.at[:, whole(y)],
                send("tap", number),
                recv("tap", y),
                (x, at(zz, yy), c),
            ).start()
        pltpu.make_async_copy(tt_buf, tap_ref.at[:, whole(y)], recv("owntap")).start()
        second_one(1)

        for number in range(16):
            sent(early_ref.at[c], send("rows", number))
        across_sent()
        sent(w_buf.at[:, ours, x], send("bw"))
        sent(w_buf.at[:, ends, x], send("xe"))
        sent(w_buf.at[:, other, x], send("xy"))
        sent(w_buf.at[:, theirs, x], send("xb"))
        sent(c_buf.at[:, ours], send("bc"))
        for number, (zz, yy) in enumerate(((ze, y), (ze, yo), (zm, yo))):
            fl = local(zz, yy)
            sent(ho_buf.at[:, fl], send("out", number * 3))
            sent(wg_buf.at[:, fl, :, left], send("out", number * 3 + 1))
            sent(wg_buf.at[:, fl, :, right], send("out", number * 3 + 2))
            sent(tt_buf, send("tap", number))
        for p in range(2):
            sent(sb_buf.at[pl.ds(2 * p, 2)], send("gc", p))
            sent(sy_buf.at[p], send("gy", p))
        sent(fo_buf.at[0], send("ge"))
        sent(fo_buf.at[1], send("gf"))
        copied(eg_ref.at[c], recv("gl"))
        arrived(eg_ref.at[co], recv("gf"))
        for kind, ref in enumerate((hid_ref, gw_ref, uw_ref)):
            copied(ref.at[:, whole(y)], recv("own", kind))
            arrived(ref.at[:, whole(yo)], recv("out", yo * 3 + kind))
        copied(tap_ref.at[:, whole(y)], recv("owntap"))
        arrived(tap_ref.at[:, whole(yo)], recv("tap", yo))


def by_halves(
    late_rows,
    early_rows,
    hidden_cot,
    gate_weight,
    up_weight,
    gate_taps,
    up_taps,
    gate_grad_sum,
    up_grad_sum,
    gate_taps_sum,
    up_taps_sum,
):
    fs_size = lax.axis_size("fs")
    rows, model = late_rows.shape
    width = gate_weight.shape[1]
    span = width // 2
    chunks = span // LANES
    half_rows = rows // 2
    scale = (rows * fs_size) ** (-0.5)
    plan = Plan(chunks)
    taps = jnp.concatenate([gate_taps, up_taps], axis=0).astype(F32)
    anywhere = pl.BlockSpec(memory_space=pl.ANY)
    vmem = pltpu.VMEM
    hidden, grad, gate_sum, up_sum, tap_sum = pl.pallas_call(
        functools.partial(layer_kernel, plan, scale),
        out_shape=(
            jax.ShapeDtypeStruct((rows, width), BF),
            jax.ShapeDtypeStruct((2, half_rows, model), BF),
            jax.ShapeDtypeStruct((rows, width), BF),
            jax.ShapeDtypeStruct((rows, width), BF),
            jax.ShapeDtypeStruct((8, width), F32),
        ),
        in_specs=[anywhere] * 5 + [pl.BlockSpec(memory_space=vmem)],
        out_specs=(anywhere,) * 5,
        scratch_shapes=[
            vmem((chunks, fs_size, 2, half_rows, 2 * LANES), BF),
            vmem((chunks, fs_size, rows, LANES), BF),
            vmem((fs_size, 2, half_rows, model), BF),
            vmem((fs_size // 2, 2, half_rows, model), BF),
            vmem((fs_size // 2, rows, fs_size * rows), BF),
            vmem((fs_size, rows, 2 * LANES), BF),
            vmem((fs_size // 2, 2, half_rows, model), F32),
            vmem((chunks, fs_size // 2, rows, LANES), BF),
            vmem((chunks, fs_size // 2, rows, 2 * LANES), BF),
            vmem((chunks, 6, 8, LANES), F32),
            vmem((8, span), F32),
            vmem((rows, 2 * LANES), BF),
            vmem((rows, 2 * LANES), BF),
            vmem((4, half_rows, model), BF),
            vmem((4, half_rows, model), BF),
            vmem((2, half_rows, model), BF),
            vmem((2, half_rows, model), BF),
            vmem((2, half_rows, model), BF),
            pltpu.SemaphoreType.DMA((plan.send_count,)),
            pltpu.SemaphoreType.DMA((plan.recv_count,)),
        ],
        compiler_params=pltpu.CompilerParams(
            has_side_effects=True, vmem_limit_bytes=67043328
        ),
    )(
        late_rows.reshape(2, half_rows, model),
        early_rows.reshape(2, half_rows, model),
        hidden_cot,
        gate_weight.reshape(2, half_rows, width),
        up_weight.reshape(2, half_rows, width),
        taps,
    )
    return (
        hidden,
        grad.reshape(rows, model),
        gate_grad_sum + gate_sum.astype(F32),
        up_grad_sum + up_sum.astype(F32),
        gate_taps_sum + scale * tap_sum[:3],
        up_taps_sum + scale * tap_sum[3:6],
    )


def solution(mesh):
    in_specs = (
        P(("rep", "fs"), None),
        P(("rep", "fs"), None),
        P(("rep", "fs"), "tp"),
        P("fs", "tp"),
        P("fs", "tp"),
        P(None, "tp"),
        P(None, "tp"),
        P(("rep", "fs"), "tp"),
        P(("rep", "fs"), "tp"),
        P("rep", "tp"),
        P("rep", "tp"),
    )
    out_specs = (
        P(("rep", "fs"), "tp"),
        P(("rep", "fs"), None),
        P(("rep", "fs"), "tp"),
        P(("rep", "fs"), "tp"),
        P("rep", "tp"),
        P("rep", "tp"),
    )
    sizes = dict(mesh.shape)

    def run(*args):
        rows = args[0].shape[0] // (sizes["rep"] * sizes["fs"])
        model = args[0].shape[1]
        width = args[3].shape[1] // sizes["tp"]
        small = rows <= 256 and model <= 2048 and width <= 2816
        even = rows % 256 == 0 and width % (2 * LANES) == 0 and model == 8 * rows
        small = small and 10 <= width // (2 * LANES) <= 11
        fits = (sizes["rep"], sizes["fs"], sizes["tp"]) == (2, 8, 2) and small and even
        return jax.shard_map(
            by_halves if fits else per_device,
            mesh=mesh,
            in_specs=in_specs,
            out_specs=out_specs,
            check_vma=False,
        )(*args)

    return run
```

```python
import functools
import math

import jax
import jax.numpy as jnp
from jax import lax
from jax.experimental import pallas as pl
from jax.experimental.pallas import tpu as pltpu
from jax.sharding import PartitionSpec as P

contract_last = (((1,), (1,)), ((), ()))
contract_first = (((0,), (0,)), ((), ()))


BF, F32 = jnp.bfloat16, jnp.float32
MESH = pl.DeviceIdType.MESH
LANES = 128
ROOT = math.sqrt(2 / math.pi)
CUBIC = 0.044715


def causal_mix(values, filter_taps):
    length = values.shape[-2]
    widths = [(0, 0)] * values.ndim
    widths[-2] = (2, 0)
    padded = jnp.pad(values, widths)
    return (
        filter_taps[0] * padded[..., 0:length, :]
        + filter_taps[1] * padded[..., 1 : length + 1, :]
        + filter_taps[2] * padded[..., 2 : length + 2, :]
    )


def mix_back(grads, filter_taps):
    length = grads.shape[-2]
    widths = [(0, 0)] * grads.ndim
    widths[-2] = (0, 2)
    padded = jnp.pad(grads, widths)
    return (
        filter_taps[2] * padded[..., 0:length, :]
        + filter_taps[1] * padded[..., 1 : length + 1, :]
        + filter_taps[0] * padded[..., 2 : length + 2, :]
    )


def tap_products(grads, values):
    length = values.shape[-2]
    widths = [(0, 0)] * values.ndim
    widths[-2] = (2, 0)
    padded = jnp.pad(values, widths)
    axes = tuple(range(values.ndim - 1))
    return jnp.stack(
        [
            jnp.sum(grads * padded[..., offset : offset + length, :], axis=axes)
            for offset in range(3)
        ]
    )


def stored(product):
    return lax.optimization_barrier(product.astype(jnp.bfloat16)).astype(jnp.float32)


def per_device(
    late_rows,
    early_rows,
    hidden_cot,
    gate_weight,
    up_weight,
    gate_taps,
    up_taps,
    gate_grad_sum,
    up_grad_sum,
    gate_taps_sum,
    up_taps_sum,
):
    row_count = late_rows.shape[0]
    width_local = gate_weight.shape[1]
    rows_scale = (row_count * lax.axis_size("fs")) ** (-0.5)
    gate_filter = gate_taps.astype(jnp.float32)
    up_filter = up_taps.astype(jnp.float32)
    joined_weight = jnp.concatenate([gate_weight, up_weight], axis=1)
    both_rows = jnp.concatenate([late_rows, early_rows], axis=0)
    whole_joined = lax.all_gather(joined_weight, "fs", axis=0, tiled=True)
    projected = jnp.dot(both_rows, whole_joined, preferred_element_type=jnp.float32)
    projected = stored(projected)
    late_gate = projected[:row_count, :width_local]
    late_up = projected[:row_count, width_local:]
    early_gate = projected[row_count:, :width_local]
    early_up = projected[row_count:, width_local:]
    late_hidden = (
        jax.nn.gelu(causal_mix(late_gate, gate_filter), approximate=True)
        * causal_mix(late_up, up_filter)
    ).astype(jnp.bfloat16)
    gate_mix = causal_mix(early_gate, gate_filter)
    up_mix = causal_mix(early_up, up_filter)
    cotangent = hidden_cot.astype(jnp.float32)
    activated, gelu_back = jax.vjp(
        lambda mixed_value: jax.nn.gelu(mixed_value, approximate=True), gate_mix
    )
    d_gate_mix = gelu_back(cotangent * up_mix)[0]
    d_up_mix = cotangent * activated
    d_gate_pre = mix_back(d_gate_mix, gate_filter).astype(jnp.bfloat16)
    d_up_pre = mix_back(d_up_mix, up_filter).astype(jnp.bfloat16)
    both_grads = jnp.concatenate([d_gate_pre, d_up_pre], axis=1)
    early_grad = lax.psum(
        lax.dot_general(
            both_grads, whole_joined, contract_last, preferred_element_type=jnp.float32
        ).astype(jnp.bfloat16),
        "tp",
    )
    summed = lax.psum_scatter(
        (
            lax.dot_general(
                early_rows, both_grads, contract_first, preferred_element_type=jnp.float32
            )
            * rows_scale
        ).astype(jnp.bfloat16),
        "fs",
        scatter_dimension=0,
        tiled=True,
    ).astype(jnp.float32)
    gate_tap_sums, up_tap_sums = lax.psum(
        (
            rows_scale * tap_products(d_gate_mix, early_gate),
            rows_scale * tap_products(d_up_mix, early_up),
        ),
        "fs",
    )
    return (
        late_hidden,
        early_grad,
        gate_grad_sum + summed[:, :width_local],
        up_grad_sum + summed[:, width_local:],
        gate_taps_sum + gate_tap_sums,
        up_taps_sum + up_tap_sums,
    )


def moved_rows(values, count):
    rows = lax.broadcasted_iota(jnp.int32, values.shape, 0)
    length = values.shape[0]
    if count > 0:
        return jnp.where(rows >= count, pltpu.roll(values, count, 0), 0.0)
    return jnp.where(rows < length + count, pltpu.roll(values, length + count, 0), 0.0)


def mixed(values, taps):
    return (
        taps[0] * moved_rows(values, 2) + taps[1] * moved_rows(values, 1) + taps[2] * values
    )


def mixed_back(values, taps):
    return (
        taps[2] * values + taps[1] * moved_rows(values, -1) + taps[0] * moved_rows(values, -2)
    )


CHUNK_RECV = ("we", "ce", "wyg", "wyu", "cy", "lg", "lu", "lc", "xe", "xy", "bw", "bc", "xb")
CHUNK_SEND = ("wyg", "wyu", "cy", "we", "ce", "xe", "xy", "bw", "bc", "xb")


class Plan:
    def __init__(self, chunks):
        self.chunks = chunks
        self.recv, self.send = {}, {}
        self.recv_count = self.send_count = 0
        self.add_recv("re", 16)
        self.add_recv("rl", 8)
        for name in CHUNK_RECV:
            self.add_recv(name, chunks)
        self.add_recv("out", 6)
        self.add_recv("own", 3)
        self.add_recv("tap", 2)
        self.add_recv("owntap", 1)
        self.add_recv("gc", 2)
        self.add_recv("gy", 2)
        self.add_recv("ge", 1)
        self.add_recv("gf", 1)
        self.add_recv("gl", 1)
        for name in CHUNK_SEND:
            self.add_send(name, 1)
        self.add_send("rows", 24)
        self.add_send("out", 9)
        self.add_send("tap", 3)
        self.add_send("gc", 2)
        self.add_send("gy", 2)
        self.add_send("ge", 1)
        self.add_send("gf", 1)

    def add_recv(self, name, count):
        self.recv[name] = self.recv_count
        self.recv_count += count

    def add_send(self, name, count):
        self.send[name] = self.send_count
        self.send_count += count


def layer_kernel(
    plan,
    scale,
    late_ref,
    early_ref,
    cot_ref,
    gate_ref,
    up_ref,
    taps_ref,
    hid_ref,
    eg_ref,
    gw_ref,
    uw_ref,
    tap_ref,
    w_buf,
    c_buf,
    re_buf,
    rl_buf,
    rt_buf,
    dp_buf,
    g_buf,
    ho_buf,
    wg_buf,
    ts_buf,
    tt_buf,
    pre_a,
    pre_b,
    sb_buf,
    sc_buf,
    sy_buf,
    ry_buf,
    fo_buf,
    send_sems,
    recv_sems,
):
    chunks = plan.chunks
    span = chunks * LANES
    model = re_buf.shape[3]
    half_rows = re_buf.shape[2]
    seq = 2 * half_rows
    x = lax.axis_index("rep")
    fs = lax.axis_index("fs")
    c = lax.axis_index("tp")
    z = fs // 2
    y = fs % 2
    hz = z // 2
    xo, yo, co = 1 - x, 1 - y, 1 - c
    zm, ze, zo = 1 + hz, 3 * hz, 2 - hz
    zoe = 3 - ze
    is_mid = z == zm
    is_end = z == ze

    def at(zz, yy):
        return zz * 2 + yy

    def local(zz, yy):
        return (zz - 2 * hz) * 2 + yy

    def recv(name, index=0):
        return recv_sems.at[plan.recv[name] + index]

    def send(name, index=0):
        return send_sems.at[plan.send[name] + index]

    def remote(src, dst, send_sem, recv_sem, target):
        return pltpu.make_async_remote_copy(
            src_ref=src,
            dst_ref=dst,
            send_sem=send_sem,
            recv_sem=recv_sem,
            device_id=target,
            device_id_type=MESH,
        )

    partner = (x, fs, co)
    across = (x, at(z, yo), c)
    facing = (xo, fs, c)
    home = (x, at(zm, y), c)
    beyond = (x, at(zo, y), c)

    def arrived(ref, sem):
        remote(ref, ref, send("rows"), sem, partner).wait_recv()

    def sent(ref, sem):
        remote(ref, ref, sem, recv("re"), partner).wait_send()

    def copied(ref, sem):
        pltpu.make_async_copy(ref, ref, sem).wait()

    def columns(side, h):
        return pl.ds(pl.multiple_of(side * span + h * LANES, LANES), LANES)

    whole = lambda side: pl.ds(pl.multiple_of(side * span, LANES), span)
    left, right = pl.ds(0, LANES), pl.ds(LANES, LANES)
    ends = pl.ds(2 * ze, 2)
    ours = pl.ds(4 * hz, 4)
    theirs = pl.ds(4 * (1 - hz), 4)

    def gather_own(h, rows):
        pltpu.make_async_copy(
            gate_ref.at[rows, :, columns(y, h)], w_buf.at[h, fs, rows, :, left], recv("lg", h)
        ).start()
        pltpu.make_async_copy(
            up_ref.at[rows, :, columns(y, h)], w_buf.at[h, fs, rows, :, right], recv("lu", h)
        ).start()
        pltpu.make_async_copy(
            cot_ref.at[:, columns(y, h)], c_buf.at[h, fs], recv("lc", h)
        ).start()

    def own_weights(h, rows):
        copied(w_buf.at[h, fs, rows, :, left], recv("lg", h))
        copied(w_buf.at[h, fs, rows, :, right], recv("lu", h))

    def own_cotangent(h):
        copied(c_buf.at[h, fs], recv("lc", h))

    def give_across(h):
        remote(
            gate_ref.at[x, :, columns(yo, h)],
            w_buf.at[h, fs, x, :, left],
            send("wyg"),
            recv("wyg", h),
            across,
        ).start()
        remote(
            up_ref.at[x, :, columns(yo, h)],
            w_buf.at[h, fs, x, :, right],
            send("wyu"),
            recv("wyu", h),
            across,
        ).start()
        remote(
            cot_ref.at[:, columns(yo, h)],
            c_buf.at[h, fs],
            send("cy"),
            recv("cy", h),
            across,
        ).start()

    def across_weights(h):
        other = at(z, yo)
        arrived(w_buf.at[h, other, x, :, left], recv("wyg", h))
        arrived(w_buf.at[h, other, x, :, right], recv("wyu", h))

    def across_cotangent(h):
        arrived(c_buf.at[h, at(z, yo)], recv("cy", h))

    def give_some(first, last):
        def one(h, _):
            give_across(h)
            return 0

        lax.fori_loop(first, last, one, 0)

    def across_sent():
        sent(gate_ref.at[x, :, whole(yo)], send("wyg"))
        sent(up_ref.at[x, :, whole(yo)], send("wyu"))
        sent(cot_ref.at[:, whole(yo)], send("cy"))

    def early_copy(src, f, half, number, target):
        return remote(
            src, re_buf.at[f, half], send("rows", number), recv("re", f * 2 + half), target
        )

    def late_copy(src, fl, half, number, target):
        return remote(
            src, rl_buf.at[fl, half], send("rows", number), recv("rl", fl * 2 + half), target
        )

    def early_here(f, half):
        arrived(re_buf.at[f, half], recv("re", f * 2 + half))

    def late_here(fl, half):
        arrived(rl_buf.at[fl, half], recv("rl", fl * 2 + half))

    @pl.when(is_end)
    def _():
        mine, other = at(ze, y), at(ze, yo)
        mine_l, other_l = local(ze, y), local(ze, yo)

        def own(h, _):
            gather_own(h, x)
            return 0

        def hand_weights(h):
            own_weights(h, x)
            across_weights(h)
            remote(
                w_buf.at[h, ends, x], w_buf.at[h, ends, x], send("we"), recv("we", h), home
            ).start()

        def hand_cotangent(h):
            own_cotangent(h)
            across_cotangent(h)
            remote(
                c_buf.at[h, ends], c_buf.at[h, ends], send("ce"), recv("ce", h), home
            ).start()

        give_across(0)
        gather_own(0, x)
        give_across(1)
        early_copy(early_ref.at[c], mine, c, 1, across).start()
        gather_own(1, x)
        hand_weights(0)
        early_copy(early_ref.at[c], mine, c, 0, home).start()
        give_some(2, 6)
        late_copy(late_ref.at[c], mine_l, c, 2, across).start()
        give_some(6, chunks)
        lax.fori_loop(2, chunks, own, 0)

        hand_weights(1)
        hand_cotangent(0)
        early_here(other, c)
        early_copy(re_buf.at[other, c], other, c, 3, home).start()
        for h in range(2, 4):
            hand_weights(h)
            hand_cotangent(h - 1)
        hand_weights(4)
        hand_weights(5)
        hand_cotangent(3)
        late_copy(late_ref.at[c], mine_l, c, 4, home).start()
        hand_weights(6)
        hand_cotangent(4)
        late_here(other_l, c)
        late_copy(rl_buf.at[other_l, c], other_l, c, 5, home).start()
        hand_weights(7)
        hand_cotangent(5)
        hand_weights(8)

        def each(h, _):
            hand_weights(h)
            hand_cotangent(h - 3)
            return 0

        lax.fori_loop(9, chunks, each, 0)
        for h in range(chunks - 3, chunks):
            hand_cotangent(h)

        sent(early_ref.at[c], send("rows", 0))
        sent(early_ref.at[c], send("rows", 1))
        sent(late_ref.at[c], send("rows", 2))
        sent(early_ref.at[c], send("rows", 3))
        sent(late_ref.at[c], send("rows", 4))
        sent(late_ref.at[c], send("rows", 5))
        across_sent()
        sent(w_buf.at[:, ends, x], send("we"))
        sent(c_buf.at[:, ends], send("ce"))

        arrived(fo_buf.at[0], recv("ge"))
        remote(fo_buf.at[0], eg_ref.at[c], send("gf"), recv("gf"), partner).start()
        keep = pltpu.make_async_copy(fo_buf.at[0], eg_ref.at[c], recv("gl"))
        keep.start()
        keep.wait()
        sent(fo_buf.at[0], send("gf"))
        arrived(eg_ref.at[co], recv("gf"))

        for side in range(2):
            arrived(hid_ref.at[:, pl.ds(side * span, span)], recv("out", side * 3))
            arrived(gw_ref.at[:, pl.ds(side * span, span)], recv("out", side * 3 + 1))
            arrived(uw_ref.at[:, pl.ds(side * span, span)], recv("out", side * 3 + 2))
            arrived(tap_ref.at[:, pl.ds(side * span, span)], recv("tap", side))

    @pl.when(is_mid)
    def _():
        mine, other = at(zm, y), at(zm, yo)
        mine_l, other_l = local(zm, y), local(zm, yo)
        both = pl.ds(0, 2)

        give_across(0)
        early_copy(early_ref.at[c], mine, c, 0, beyond).start()
        early_copy(early_ref.at[c], mine, c, 1, across).start()
        give_across(1)
        gather_own(0, both)
        keep_early = pltpu.make_async_copy(early_ref, re_buf.at[mine], recv("re", mine * 2))
        keep_late = pltpu.make_async_copy(late_ref, rl_buf.at[mine_l], recv("rl", mine_l * 2))
        keep_early.start()

        def own(h, _):
            gather_own(h, both)
            return 0

        lax.fori_loop(1, chunks, own, 0)
        keep_late.start()

        def clear(fl, _):
            g_buf[fl] = jnp.zeros_like(g_buf[0])
            return 0

        lax.fori_loop(0, 4, clear, 0)

        def turn(f):
            def one(fl, _):
                cols = pl.ds(pl.multiple_of((4 * hz + fl) * seq, LANES), seq)
                block = re_buf[f, :, :, cols].reshape(seq, seq)
                rt_buf[fl, :, pl.ds(pl.multiple_of(f * seq, LANES), seq)] = block.T
                return 0

            lax.fori_loop(0, 4, one, 0)

        def swap_early(f, number):
            early_copy(re_buf.at[f, c], f, c, number, partner).start()

        def swap_late(fl, number):
            late_copy(rl_buf.at[fl, c], fl, c, number, partner).start()

        def pass_weights(h):
            own_weights(h, both)
            across_weights(h)
            arrived(w_buf.at[h, ends, x], recv("we", h))
            remote(
                w_buf.at[h, ours, x], w_buf.at[h, ours, x], send("bw"), recv("bw", h), beyond
            ).start()
            remote(
                w_buf.at[h, ends, x], w_buf.at[h, ends, x], send("xe"), recv("xe", h), facing
            ).start()
            remote(
                w_buf.at[h, other, x], w_buf.at[h, other, x], send("xy"), recv("xy", h), facing
            ).start()

        def cotangent_here(h):
            own_cotangent(h)
            across_cotangent(h)
            arrived(c_buf.at[h, ends], recv("ce", h))

        def pass_cotangent(h):
            remote(
                c_buf.at[h, ours], c_buf.at[h, ours], send("bc"), recv("bc", h), beyond
            ).start()

        def pass_over(h):
            arrived(w_buf.at[h, theirs, x], recv("bw", h))
            remote(
                w_buf.at[h, theirs, x], w_buf.at[h, theirs, x], send("xb"), recv("xb", h), facing
            ).start()

        def weights_here(h):
            arrived(w_buf.at[h, ends, xo], recv("xe", h))
            arrived(w_buf.at[h, other, xo], recv("xy", h))
            arrived(w_buf.at[h, theirs, xo], recv("xb", h))

        near, far = at(zo, y), at(zoe, y)
        near_o, far_o = at(zo, yo), at(zoe, yo)
        end_y, end_o = at(ze, y), at(ze, yo)
        late_others = (local(ze, y), local(ze, yo), other_l)

        pass_weights(0)
        early_here(near, c)
        early_copy(re_buf.at[near, c], near, c, 6, across).start()
        give_across(2)
        swap_early(near, 7)
        early_here(other, c)
        swap_early(other, 5)
        keep_early.wait()
        turn(mine)
        early_here(end_y, c)
        early_copy(re_buf.at[end_y, c], end_y, c, 2, beyond).start()
        swap_early(end_y, 3)
        pass_weights(1)
        cotangent_here(0)
        pass_cotangent(0)
        pass_over(0)
        for f in (other, near):
            early_here(f, co)
            turn(f)
        early_here(far, c)
        early_copy(re_buf.at[far, c], far, c, 8, across).start()
        give_some(3, 5)
        late_copy(late_ref.at[c], mine_l, c, 12, across).start()
        give_some(5, chunks)
        swap_early(far, 9)
        early_here(end_y, co)
        turn(end_y)
        early_here(end_o, c)
        swap_early(end_o, 4)
        pass_weights(2)
        early_here(end_o, co)
        turn(end_o)

        block = 16

        def by_rows(work):
            def one(i, _):
                work(pl.ds(pl.multiple_of(i * block, block), block))
                return 0

            lax.fori_loop(0, half_rows // block, one, 0)

        def base(p):
            return 2 * hz if p == 0 else 2 * (1 - hz)

        def narrow_all():
            for p in range(2):

                def narrow(rows, p=p):
                    for side in range(2):
                        sb_buf[2 * p + side, rows] = g_buf[base(p) + side, co, rows].astype(BF)

                by_rows(narrow)
                pair = pl.ds(2 * p, 2)
                remote(
                    sb_buf.at[pair], sc_buf.at[pair], send("gc", p), recv("gc", p), partner
                ).start()

        def first_all():
            for p in range(2):
                arrived(sc_buf.at[pl.ds(2 * p, 2)], recv("gc", p))

                def first(rows, p=p):
                    sy_buf[p, rows] = (
                        g_buf[base(p) + yo, c, rows] + sc_buf[2 * p + yo, rows].astype(F32)
                    ).astype(BF)

                by_rows(first)
                remote(sy_buf.at[p], ry_buf.at[p], send("gy", p), recv("gy", p), across).start()

        def second_one(p):
            arrived(ry_buf.at[p], recv("gy", p))

            def second(rows):
                fo_buf[p, rows] = (
                    g_buf[base(p) + y, c, rows]
                    + sc_buf[2 * p + y, rows].astype(F32)
                    + ry_buf[p, rows].astype(F32)
                ).astype(BF)

            by_rows(second)
            if p == 0:
                remote(
                    fo_buf.at[0],
                    fo_buf.at[0],
                    send("ge"),
                    recv("ge"),
                    (x, at(ze, y), c),
                ).start()
            else:
                remote(fo_buf.at[1], eg_ref.at[c], send("gf"), recv("gf"), partner).start()
                pltpu.make_async_copy(fo_buf.at[1], eg_ref.at[c], recv("gl")).start()

        pres = (pre_a, pre_b)
        lag = 3

        def step(t, _):
            def taps_of(h):
                cols = columns(y, h)
                gate = [taps_ref[j : j + 1, cols] for j in range(3)]
                up = [taps_ref[j + 3 : j + 4, cols] for j in range(3)]
                return gate, up

            def project(rows, h, number):
                pres[number % 2][...] = jnp.dot(
                    rows.reshape(seq, model),
                    w_buf[h].reshape(model, 2 * LANES),
                    preferred_element_type=F32,
                ).astype(BF)

            def early(h, f, number, taps):
                gate_taps, up_taps = taps
                pre = pres[number % 2]
                gate_pre = pre[:, :LANES].astype(F32)
                up_pre = pre[:, LANES:].astype(F32)
                gate_mix = mixed(gate_pre, gate_taps)
                up_mix = mixed(up_pre, up_taps)
                cot = c_buf[h, f].astype(F32)
                square = gate_mix * gate_mix
                tanh = jnp.tanh(ROOT * gate_mix * (1.0 + CUBIC * square))
                half = 0.5 * (1.0 + tanh)
                slope = half + 0.5 * gate_mix * (1.0 - tanh * tanh) * (
                    ROOT * (1.0 + 3 * CUBIC * square)
                )
                d_gate = cot * up_mix * slope
                d_up = cot * (gate_mix * half)
                sums = []
                for grad, value in ((d_gate, gate_pre), (d_up, up_pre)):
                    for j in range(3):
                        other_value = moved_rows(value, 2 - j) if j < 2 else value
                        product = grad * other_value
                        sums.append(product.reshape(seq // 8, 8, LANES).sum(0))
                back = jnp.concatenate(
                    [
                        mixed_back(d_gate, gate_taps).astype(BF),
                        mixed_back(d_up, up_taps).astype(BF),
                    ],
                    axis=1,
                )
                return back, jnp.stack(sums)

            def late(h, fl, number, taps):
                gate_taps, up_taps = taps
                pre = pres[number % 2]
                gate_mix = mixed(pre[:, :LANES].astype(F32), gate_taps)
                up_mix = mixed(pre[:, LANES:].astype(F32), up_taps)
                tanh = jnp.tanh(ROOT * gate_mix * (1.0 + CUBIC * gate_mix * gate_mix))
                ho_buf[h, fl] = (0.5 * gate_mix * (1.0 + tanh) * up_mix).astype(BF)

            def input_grad(h, n):
                term = lax.dot_general(
                    wg_buf[h].reshape(4 * seq, 2 * LANES),
                    w_buf[h, n].reshape(seq, 2 * LANES),
                    contract_last,
                    preferred_element_type=F32,
                )
                cols = pl.ds(n * seq, seq)
                g_buf[:, :, :, cols] += term.reshape(4, 2, half_rows, seq)

            def give_out(h, kinds):
                cols = columns(y, h)
                for kind in kinds:
                    lanes = right if kind == 2 else left
                    dst = (hid_ref, gw_ref, uw_ref)[kind]

                    def src(fl):
                        if kind == 0:
                            return ho_buf.at[h, fl]
                        return wg_buf.at[h, fl, :, lanes]

                    for number, (zz, yy) in enumerate(((ze, y), (ze, yo), (zm, yo))):
                        remote(
                            src(local(zz, yy)),
                            dst.at[:, cols],
                            send("out", number * 3 + kind),
                            recv("out", y * 3 + kind),
                            (x, at(zz, yy), c),
                        ).start()
                    pltpu.make_async_copy(
                        src(mine_l), dst.at[:, cols], recv("own", kind)
                    ).start()

            def late_chunk(h, n_grads=None):
                taps = taps_of(h)
                project(rl_buf[0], h, 0)
                for fl in range(4):
                    if fl < 3:
                        project(rl_buf[fl + 1], h, fl + 1)
                    late(h, fl, fl, taps)
                    if n_grads is not None:
                        input_grad(n_grads, 2 * fl)
                        input_grad(n_grads, 2 * fl + 1)
                give_out(h, (0,))

            @pl.when(t < chunks)
            def _():
                weights_here(t)

                @pl.when(t + 1 < chunks)
                def _():
                    pass_over(t + 1)

                taps = taps_of(t)
                first = 4 * hz
                project(re_buf[first], t, 0)
                for fl in range(4):
                    if fl < 3:
                        project(re_buf[first + fl + 1], t, fl + 1)
                    back, sums = early(t, first + fl, fl, taps)
                    wg_buf[t, fl] = back
                    if fl == 0:
                        ts_buf[t] = sums
                    else:
                        ts_buf[t] += sums

            @pl.when(t == 0)
            def _():
                early_here(near_o, c)
                swap_early(near_o, 10)
                early_here(far, co)
                turn(far)

            @pl.when(t == 1)
            def _():
                early_here(far_o, c)
                swap_early(far_o, 11)
                early_here(near_o, co)
                turn(near_o)
                early_here(far_o, co)
                turn(far_o)

            @pl.when(t == 4)
            def _():
                for fl, number in zip(late_others, (13, 14, 15)):
                    late_here(fl, c)
                    swap_late(fl, number)
                keep_late.wait()
                for fl in late_others:
                    late_here(fl, co)

            late_first = jnp.where(t < 8, 2 * (t - 4), t)

            @pl.when((t < 4) | (t == chunks - 1))
            def _():
                for n in range(8):
                    input_grad(t, n)

            @pl.when(t == chunks - 1)
            def _():
                narrow_all()

            @pl.when((t >= 4) & (t < chunks - 1))
            def _():
                late_chunk(late_first, t)

            @pl.when(((t >= 4) & (t < 8)) | (t == chunks - 1))
            def _():
                late_chunk(jnp.where(t < 8, late_first + 1, t))

            @pl.when(t == chunks - 1)
            def _():
                first_all()

            @pl.when(t == chunks + 1)
            def _():
                second_one(0)

            @pl.when(t == 0)
            def _():
                cotangent_here(1)
                pass_cotangent(1)

            @pl.when(t == 1)
            def _():
                pass_weights(3)

            @pl.when((t >= 1) & (t != 4))
            def _():
                h = jnp.where(t < 4, t - 1, t - lag + 1)
                arrived(c_buf.at[h, theirs], recv("bc", h))
                for fl in range(4):
                    dp_buf[4 * hz + fl] = wg_buf[h, fl]
                taps = taps_of(h)
                first = 4 * (1 - hz)
                total = None
                project(re_buf[first], h, 0)
                for fl in range(4):
                    if fl < 3:
                        project(re_buf[first + fl + 1], h, fl + 1)
                    back, sums = early(h, first + fl, fl, taps)
                    dp_buf[first + fl] = back
                    total = sums if total is None else total + sums
                total = ts_buf[h] + total
                here = pl.ds(pl.multiple_of(h * LANES, LANES), LANES)
                tt_buf[pl.ds(0, 6), here] = jnp.sum(total, axis=1)
                for fl in range(4):
                    product = jnp.dot(
                        rt_buf[fl],
                        dp_buf[...].reshape(8 * seq, 2 * LANES),
                        preferred_element_type=F32,
                    )
                    wg_buf[h, fl] = (product * scale).astype(BF)
                give_out(h, (1, 2))

            @pl.when((t >= 1) & (t + 3 < chunks))
            def _():
                pass_weights(t + 3)

            @pl.when((t >= 1) & (t + 1 < chunks))
            def _():
                cotangent_here(t + 1)
                pass_cotangent(t + 1)

            return 0

        lax.fori_loop(0, chunks + lag - 1, step, 0)
        for number, (zz, yy) in enumerate(((ze, y), (ze, yo), (zm, yo))):
            remote(
                tt_buf,
                tap_ref.at[:, whole(y)],
                send("tap", number),
                recv("tap", y),
                (x, at(zz, yy), c),
            ).start()
        pltpu.make_async_copy(tt_buf, tap_ref.at[:, whole(y)], recv("owntap")).start()
        second_one(1)

        for number in range(16):
            sent(early_ref.at[c], send("rows", number))
        across_sent()
        sent(w_buf.at[:, ours, x], send("bw"))
        sent(w_buf.at[:, ends, x], send("xe"))
        sent(w_buf.at[:, other, x], send("xy"))
        sent(w_buf.at[:, theirs, x], send("xb"))
        sent(c_buf.at[:, ours], send("bc"))
        for number, (zz, yy) in enumerate(((ze, y), (ze, yo), (zm, yo))):
            fl = local(zz, yy)
            sent(ho_buf.at[:, fl], send("out", number * 3))
            sent(wg_buf.at[:, fl, :, left], send("out", number * 3 + 1))
            sent(wg_buf.at[:, fl, :, right], send("out", number * 3 + 2))
            sent(tt_buf, send("tap", number))
        for p in range(2):
            sent(sb_buf.at[pl.ds(2 * p, 2)], send("gc", p))
            sent(sy_buf.at[p], send("gy", p))
        sent(fo_buf.at[0], send("ge"))
        sent(fo_buf.at[1], send("gf"))
        copied(eg_ref.at[c], recv("gl"))
        arrived(eg_ref.at[co], recv("gf"))
        for kind, ref in enumerate((hid_ref, gw_ref, uw_ref)):
            copied(ref.at[:, whole(y)], recv("own", kind))
            arrived(ref.at[:, whole(yo)], recv("out", yo * 3 + kind))
        copied(tap_ref.at[:, whole(y)], recv("owntap"))
        arrived(tap_ref.at[:, whole(yo)], recv("tap", yo))


def by_halves(
    late_rows,
    early_rows,
    hidden_cot,
    gate_weight,
    up_weight,
    gate_taps,
    up_taps,
    gate_grad_sum,
    up_grad_sum,
    gate_taps_sum,
    up_taps_sum,
):
    fs_size = lax.axis_size("fs")
    rows, model = late_rows.shape
    width = gate_weight.shape[1]
    span = width // 2
    chunks = span // LANES
    half_rows = rows // 2
    scale = (rows * fs_size) ** (-0.5)
    plan = Plan(chunks)
    taps = jnp.concatenate([gate_taps, up_taps], axis=0).astype(F32)
    anywhere = pl.BlockSpec(memory_space=pl.ANY)
    vmem = pltpu.VMEM
    hidden, grad, gate_sum, up_sum, tap_sum = pl.pallas_call(
        functools.partial(layer_kernel, plan, scale),
        out_shape=(
            jax.ShapeDtypeStruct((rows, width), BF),
            jax.ShapeDtypeStruct((2, half_rows, model), BF),
            jax.ShapeDtypeStruct((rows, width), BF),
            jax.ShapeDtypeStruct((rows, width), BF),
            jax.ShapeDtypeStruct((8, width), F32),
        ),
        in_specs=[anywhere] * 5 + [pl.BlockSpec(memory_space=vmem)],
        out_specs=(anywhere,) * 5,
        scratch_shapes=[
            vmem((chunks, fs_size, 2, half_rows, 2 * LANES), BF),
            vmem((chunks, fs_size, rows, LANES), BF),
            vmem((fs_size, 2, half_rows, model), BF),
            vmem((fs_size // 2, 2, half_rows, model), BF),
            vmem((fs_size // 2, rows, fs_size * rows), BF),
            vmem((fs_size, rows, 2 * LANES), BF),
            vmem((fs_size // 2, 2, half_rows, model), F32),
            vmem((chunks, fs_size // 2, rows, LANES), BF),
            vmem((chunks, fs_size // 2, rows, 2 * LANES), BF),
            vmem((chunks, 6, 8, LANES), F32),
            vmem((8, span), F32),
            vmem((rows, 2 * LANES), BF),
            vmem((rows, 2 * LANES), BF),
            vmem((4, half_rows, model), BF),
            vmem((4, half_rows, model), BF),
            vmem((2, half_rows, model), BF),
            vmem((2, half_rows, model), BF),
            vmem((2, half_rows, model), BF),
            pltpu.SemaphoreType.DMA((plan.send_count,)),
            pltpu.SemaphoreType.DMA((plan.recv_count,)),
        ],
        compiler_params=pltpu.CompilerParams(
            has_side_effects=True, vmem_limit_bytes=67043328
        ),
    )(
        late_rows.reshape(2, half_rows, model),
        early_rows.reshape(2, half_rows, model),
        hidden_cot,
        gate_weight.reshape(2, half_rows, width),
        up_weight.reshape(2, half_rows, width),
        taps,
    )
    return (
        hidden,
        grad.reshape(rows, model),
        gate_grad_sum + gate_sum.astype(F32),
        up_grad_sum + up_sum.astype(F32),
        gate_taps_sum + scale * tap_sum[:3],
        up_taps_sum + scale * tap_sum[3:6],
    )


def solution(mesh):
    in_specs = (
        P(("rep", "fs"), None),
        P(("rep", "fs"), None),
        P(("rep", "fs"), "tp"),
        P("fs", "tp"),
        P("fs", "tp"),
        P(None, "tp"),
        P(None, "tp"),
        P(("rep", "fs"), "tp"),
        P(("rep", "fs"), "tp"),
        P("rep", "tp"),
        P("rep", "tp"),
    )
    out_specs = (
        P(("rep", "fs"), "tp"),
        P(("rep", "fs"), None),
        P(("rep", "fs"), "tp"),
        P(("rep", "fs"), "tp"),
        P("rep", "tp"),
        P("rep", "tp"),
    )
    sizes = dict(mesh.shape)

    def run(*args):
        rows = args[0].shape[0] // (sizes["rep"] * sizes["fs"])
        model = args[0].shape[1]
        width = args[3].shape[1] // sizes["tp"]
        small = rows <= 256 and model <= 2048 and width <= 2816
        even = rows % 256 == 0 and width % (2 * LANES) == 0 and model == 8 * rows
        small = small and 10 <= width // (2 * LANES) <= 11
        fits = (sizes["rep"], sizes["fs"], sizes["tp"]) == (2, 8, 2) and small and even
        return jax.shard_map(
            by_halves if fits else per_device,
            mesh=mesh,
            in_specs=in_specs,
            out_specs=out_specs,
            check_vma=False,
        )(*args)

    return run
```
